512 devices in a mesh: dp: 4 (over x), kv: 64 (over z, y), tp: 2 (over core).
Axes of the slice: x: 4, y: 8, z: 8, core: 2. Of those that a mesh axis runs over, the one named last changes fastest.
Arguments:
- tokens: bfloat16 [16, 4096], P('dp', ('kv', 'tp')), may hold values from -11 to 11
- attn_gain: float32 [4096], replicated, may hold values from 0.1 to 1.9
- query_weight: bfloat16 [4096, 4096], P('kv', 'tp'), may hold values from -0.09375 to 0.09375
- key_cache: bfloat16 [16, 16384, 2, 128], P('dp', 'kv', 'tp'), may hold values from -820 to 820
- value_cache: bfloat16 [16, 16384, 2, 128], P('dp', 'kv', 'tp'), may hold values from -6 to 6
- head_lambda: float32 [32], P('tp'), may hold values from 0.3 to 0.8
- head_gain: float32 [128], replicated, may hold values from 0.1 to 1.9
- out_weight: bfloat16 [4096, 4096], P('kv', 'tp'), may hold values from -0.09375 to 0.09375
- mlp_gain: float32 [4096], replicated, may hold values from 0.1 to 1.9
- gate_weight: bfloat16 [11264, 4096], P(('kv', 'tp')), may hold values from -0.09375 to 0.09375
- up_weight: bfloat16 [11264, 4096], P(('kv', 'tp')), may hold values from -0.09375 to 0.09375
- down_weight: bfloat16 [11264, 4096], P(('kv', 'tp')), may hold values from -0.21875 to 0.21875
Outputs:
- mixed: bfloat16 [16, 4096], P('dp', ('kv', 'tp'))
The draws below stay inside these ranges and needn't reach their ends.
All inputs are finite; a program needn't handle non-finite values.
Results may differ from the reference program's by a relative error of at most 0.02.
The reference program's roundings to bfloat16 on the way (of `scaled`, `rotated`, `probs`, `head_out`, `normed` and `hidden`) count: a program that leaves them out, or rounds other values in their place, can miss the bound.
Values may be sent and summed in bfloat16 or wider, within the bound.
No kernel may reach another device: no remote copies, remote signals or barrier semaphores. Data moves between devices by JAX's collectives and lax.ppermute only.
A program may use at most 64 MiB of HBM per device.

```python
import jax
import jax.numpy as jnp
from jax import lax

D = 4096
HEADS = 32
KV_HEADS = 2
HEAD = 64
FF = 11264
VALUE = 128
GROUP = 16
BATCH = 16
CACHE_LEN = 16384
N_TP = 2


def draw_tokens(key, part):
    column_scale = 10.0 ** (jnp.arange(D, dtype=jnp.float32) / D - 0.5)
    row_scale = 10.0 ** (jax.random.uniform(jax.random.fold_in(key, 21), (BATCH, 1), jnp.float32) - 0.5)
    base = jnp.clip(jax.random.normal(jax.random.fold_in(key, 24), (BATCH, D), jnp.float32), -4.0, 4.0)
    return (0.25 * row_scale * column_scale * base).astype(jnp.bfloat16)


def draw_key_cache(key, part):
    shape = (BATCH, CACHE_LEN, KV_HEADS, 2 * HEAD)
    base = jnp.clip(jax.random.normal(jax.random.fold_in(key, 11), shape, jnp.float32), -4.0, 4.0)
    spots = jax.random.randint(jax.random.fold_in(key, 12), (BATCH, 1, KV_HEADS, 4), 0, CACHE_LEN - 1)
    strength = jax.random.uniform(jax.random.fold_in(key, 13), (BATCH, 1, KV_HEADS, 4), jnp.float32, 100.0, 200.0)
    flips = jax.random.randint(jax.random.fold_in(key, 14), (BATCH, 1, KV_HEADS, 4), 0, 2)
    signed = strength * (2.0 * flips.astype(jnp.float32) - 1.0)
    place = jnp.arange(CACHE_LEN, dtype=jnp.int32).reshape(1, CACHE_LEN, 1, 1)
    hits = place == spots
    factor = jnp.sum(jnp.where(hits, signed, 0.0), axis=-1, keepdims=True)
    marked = jnp.any(hits, axis=-1, keepdims=True)
    follow_factor = jnp.roll(factor, 1, axis=1)
    follow = jnp.logical_and(jnp.roll(marked, 1, axis=1), jnp.logical_not(marked))
    lifted = jnp.roll(base, 1, axis=1)
    planted = jnp.where(marked, factor * base, jnp.where(follow, 1.01 * follow_factor * lifted, 2.0 * base))
    return planted.astype(jnp.bfloat16)


def spiked(array, stream_key, source, target, blocks, factor):
    def block_of(dim):
        return (jnp.arange(array.shape[dim]) // (array.shape[dim] // blocks)).reshape((-1,) + (1,) * (array.ndim - 1 - dim))

    one_side = jax.random.permutation(stream_key, blocks)[block_of(target)]
    second = (block_of(target) + blocks // 2) % blocks
    return jnp.where((block_of(source) == one_side) | (block_of(source) == second), factor * array, array)


def levels(stream_key, dims, split, least, high):
    loudness, own = 1.0, jax.random.fold_in(stream_key, 6)
    for axis_at, blocks in split:
        steps = jnp.exp(jax.random.uniform(jax.random.fold_in(own, axis_at), (blocks,), jnp.float32, least / len(split), high / len(split)))
        loudness = loudness * jnp.repeat(steps, dims[axis_at] // blocks).reshape([-1 if axis == axis_at else 1 for axis in range(len(dims))])
    return loudness


def gaussian(own_key, dims, scale, most, cuts=(), kind=jnp.bfloat16):
    result = scale * jax.random.normal(own_key, dims, jnp.float32)
    if cuts:
        result = result * levels(own_key, dims, cuts, -0.22, 0.18)
    return jnp.clip(result, -most, most).astype(kind)


def gaussian_with(stream_key, dims, deviation, limit, pieces, heavy, kind=jnp.bfloat16):
    values = deviation * jax.random.normal(stream_key, dims, jnp.float32)
    if pieces:
        values = values * levels(stream_key, dims, pieces, -0.22, 0.18)
    return jnp.clip(spiked(values, jax.random.fold_in(stream_key, 3), *heavy), -limit, limit).astype(kind)


def setup_inputs(seed: int = 0) -> dict:
    key_of = jax.random.split(jax.random.key(seed), 13)
    return {
        "tokens": draw_tokens(jax.random.fold_in(key_of[12], 71), 0),
        "attn_gain": jnp.clip(1.0 + 0.18 * jax.random.normal(key_of[1], (D,), jnp.float32), 0.1, 1.9),
        "query_weight": gaussian(key_of[2], (D, HEADS * 2 * HEAD), D ** -0.5, 0.09375, ((0, 64), (1, 2))),
        "key_cache": draw_key_cache(jax.random.fold_in(key_of[12], 71), 0),
        "value_cache": gaussian(key_of[4], (BATCH, CACHE_LEN, KV_HEADS, VALUE), 1.0, 6.0, ((0, 4), (1, 64), (2, 2))),
        "head_lambda": jnp.clip(0.3 + 0.5 * jax.random.uniform(key_of[5], (HEADS,), jnp.float32) ** levels(key_of[5], (HEADS,), ((0, 2),), -0.2, 0.2), 0.3, 0.8),
        "head_gain": jnp.clip(1.0 + 0.18 * jax.random.normal(key_of[6], (VALUE,), jnp.float32), 0.1, 1.9),
        "out_weight": gaussian(key_of[7], (D, HEADS * VALUE), (HEADS * VALUE) ** -0.5, 0.09375, ((0, 64), (1, 2))),
        "mlp_gain": jnp.clip(1.0 + 0.18 * jax.random.normal(key_of[8], (D,), jnp.float32), 0.1, 1.9),
        "gate_weight": gaussian(key_of[9], (FF, D), D ** -0.5, 0.09375, ((0, 128),)),
        "up_weight": gaussian(key_of[10], (FF, D), D ** -0.5, 0.09375, ((0, 128),)),
        "down_weight": gaussian_with(key_of[11], (FF, D), FF ** -0.5, 0.21875, ((0, 128),), (0, 1, 128, 5.5)),
    }


EPS = 1e-06
THETA = 10000.0

def rotate(vector, position):
    half_len = vector.shape[-1] // 2
    inv_freq = 1.0 / THETA ** (jnp.arange(half_len, dtype=jnp.float32) / half_len)
    angles = position * inv_freq
    cos_table = jnp.cos(angles)
    sin_table = jnp.sin(angles)
    first_half = vector[..., :half_len]
    second_half = vector[..., half_len:]
    return jnp.concatenate([first_half * cos_table - second_half * sin_table, second_half * cos_table + first_half * sin_table], axis=-1)

def reference(tokens, attn_gain, query_weight, key_cache, value_cache, head_lambda, head_gain, out_weight, mlp_gain, gate_weight, up_weight, down_weight):
    as_float = tokens.astype(jnp.float32)
    mean_square = lax.optimization_barrier(jnp.mean(as_float * as_float, axis=-1, keepdims=True))
    scaled = (as_float * attn_gain).astype(jnp.bfloat16)
    queries = jnp.dot(scaled, query_weight, preferred_element_type=jnp.float32) * lax.rsqrt(mean_square + EPS)
    queries = queries.reshape(BATCH, HEADS, 2, HEAD)
    rotated = rotate(queries, jnp.float32(CACHE_LEN)).astype(jnp.bfloat16)
    lam_grid = head_lambda.reshape(KV_HEADS, GROUP, 1)

    def attend(item):
        query_row, key_rows, value_rows = item
        query_grid = query_row.reshape(KV_HEADS, GROUP, 2, HEAD).astype(jnp.float32)
        key_grid = key_rows.reshape(CACHE_LEN, KV_HEADS, 2, HEAD).astype(jnp.float32)
        scores = jnp.einsum('kgch,lkch->kgcl', query_grid, key_grid) * HEAD ** (-0.5)
        top_score = lax.optimization_barrier(jnp.max(scores, axis=-1, keepdims=True))
        weights_exp = jnp.exp(scores - top_score)
        exp_total = lax.optimization_barrier(jnp.sum(weights_exp, axis=-1))
        probs = weights_exp.astype(jnp.bfloat16).astype(jnp.float32)
        weighted = jnp.einsum('kgcl,lkv->kgcv', probs, value_rows.astype(jnp.float32))
        attended = weighted / exp_total[..., None]
        difference = attended[:, :, 0] - lam_grid * attended[:, :, 1]
        head_norm = lax.rsqrt(lax.optimization_barrier(jnp.mean(difference * difference, axis=-1, keepdims=True)) + EPS)
        head_out = difference * head_norm * head_gain
        return head_out.reshape(HEADS * VALUE).astype(jnp.bfloat16)
    head_out = lax.map(attend, (rotated, key_cache, value_cache))
    group_rows = HEADS * VALUE // N_TP
    attention = jnp.zeros((BATCH, D), jnp.float32)
    for tp_slot in range(N_TP):
        block_out = lax.dot_general(head_out[:, tp_slot * group_rows:(tp_slot + 1) * group_rows], out_weight[:, tp_slot * group_rows:(tp_slot + 1) * group_rows], (((1,), (1,)), ((), ())), preferred_element_type=jnp.float32).astype(jnp.bfloat16)
        attention = attention + block_out.astype(jnp.float32)
    stream = as_float + attention
    stream_square = lax.optimization_barrier(jnp.mean(stream * stream, axis=-1, keepdims=True))
    normed = (stream * lax.rsqrt(stream_square + EPS) * mlp_gain).astype(jnp.bfloat16)
    gate_out = lax.dot_general(normed, gate_weight, (((1,), (1,)), ((), ())), preferred_element_type=jnp.float32)
    up_out = lax.dot_general(normed, up_weight, (((1,), (1,)), ((), ())), preferred_element_type=jnp.float32)
    hidden = (jax.nn.silu(gate_out) * up_out).astype(jnp.bfloat16)
    down_out = jnp.dot(hidden, down_weight, preferred_element_type=jnp.float32)
    return (stream + down_out).astype(jnp.bfloat16)
```

```python
import jax
import jax.numpy as jnp
from jax import lax
from jax.experimental import pallas as pl
from jax.experimental.pallas import tpu as pltpu
from jax.sharding import Mesh
from jax.sharding import PartitionSpec as P

KV = ("kv_0", "kv_1")
KV_TP = ("kv_0", "kv_1", "tp")
EPS = 1e-06
THETA = 10000.0
F32 = jnp.float32
BF16 = jnp.bfloat16
SHAPE = jax.ShapeDtypeStruct


def lanes(shape):
    return lax.broadcasted_iota(jnp.int32, shape, len(shape) - 1)


def rows(shape):
    return lax.broadcasted_iota(jnp.int32, shape, len(shape) - 2)


def inner_last(left, right):
    return lax.dot_general(left, right, (((1,), (1,)), ((), ())), preferred_element_type=F32)


def shared(block, axis):
    copies = jnp.broadcast_to(block, (lax.axis_size(axis), *block.shape))
    return lax.all_to_all(copies, axis, 0, 0, tiled=True)


def query_kernel(tp_ref, own_ref, other_ref, gain_ref, weight_ref, out_ref):
    own = own_ref[...].astype(F32)
    other = other_ref[...].astype(F32)
    both = jnp.concatenate([own, other, own, other], axis=1)
    x = jnp.where(tp_ref[0] == 0, both[:, :64], both[:, 32:96])
    square = jnp.sum(x * x, axis=1, keepdims=True)
    scaled = (x * gain_ref[...]).astype(BF16)
    q = jnp.dot(scaled, weight_ref[...], preferred_element_type=F32)
    for h in range(16):
        out_ref[4 * h : 4 * h + 4, :] = q[:, 128 * h : 128 * h + 128]
    wide = jnp.broadcast_to(square, (4, 128))
    out_ref[64:68, :] = wide
    out_ref[68:72, :] = wide


def pack(values, lse):
    high = lse.astype(BF16).astype(F32)
    mid = (lse - high).astype(BF16).astype(F32)
    low = lse - high - mid
    at = rows((16, 128))
    tail = jnp.where(at == 0, high, jnp.where(at == 1, mid, jnp.where(at == 2, low, 0.0)))
    return values.astype(BF16), tail.astype(BF16)


def attend_kernel(parts_ref, cos_ref, sin_ref, key_ref, value_ref, out_ref):
    total = parts_ref[0]
    for k in range(1, 8):
        total = total + parts_ref[k]
    scale = lax.rsqrt(total[64:72] * (1.0 / 4096) + EPS)
    q = (total[:64].reshape(8, 8, 128) * scale[None]).reshape(64, 128)
    lane = lanes((64, 128))
    swapped = jnp.where(lane % 64 < 32, pltpu.roll(q, 96, 1), pltpu.roll(q, 32, 1))
    turned = q * cos_ref[...] + swapped * sin_ref[...]
    both = jnp.concatenate(
        [jnp.where(lane < 64, turned, 0.0), jnp.where(lane < 64, 0.0, turned)], axis=0
    ).astype(BF16)
    row = rows((128, 256)) % 4
    scores = inner_last(both, key_ref[0])
    for b in range(1, 4):
        scores = jnp.where(row == b, inner_last(both, key_ref[b]), scores)
    scores = scores * 0.125
    peak = jnp.max(scores, axis=1, keepdims=True)
    e = jnp.exp(scores - peak)
    total_e = jnp.sum(e, axis=1, keepdims=True)
    probs = e.astype(BF16)
    row_v = rows((128, 128)) % 4
    value = jnp.dot(probs, value_ref[0], preferred_element_type=F32)
    for b in range(1, 4):
        value = jnp.where(
            row_v == b, jnp.dot(probs, value_ref[b], preferred_element_type=F32), value
        )
    value = value / total_e
    lse = peak + jnp.log(total_e)
    eye = rows((128, 128)) == lanes((128, 128))
    lse_row = jnp.sum(jnp.where(eye, lse, 0.0), axis=0, keepdims=True)
    out_ref[:128, :], out_ref[128:, :] = pack(value, lse_row)


def merged(parts_ref):
    tails = []
    for k in range(8):
        tail = parts_ref[k, 128:, :].astype(F32)
        tails.append(tail[0:1] + tail[1:2] + tail[2:3])
    lse = jnp.concatenate(tails, axis=0)
    peak = jnp.max(lse, axis=0, keepdims=True)
    e = jnp.exp(lse - peak)
    total = jnp.sum(e, axis=0, keepdims=True)
    share = (e / total).T
    value = share[:, 0:1] * parts_ref[0, :128, :].astype(F32)
    for k in range(1, 8):
        value = value + share[:, k : k + 1] * parts_ref[k, :128, :].astype(F32)
    return value, peak + jnp.log(total)


def merge_kernel(parts_ref, out_ref):
    out_ref[:128, :], out_ref[128:, :] = pack(*merged(parts_ref))


def project_kernel(tp_ref, parts_ref, lam_ref, gain_ref, weight_ref, own_ref, out_ref, heads_ref):
    value, _ = merged(parts_ref)
    difference = value[:64] - lam_ref[...] * value[64:]
    norm = lax.rsqrt(jnp.mean(difference * difference, axis=1, keepdims=True) + EPS)
    heads_ref[...] = difference * norm * gain_ref[...]
    head_out = jnp.concatenate([heads_ref[4 * h : 4 * h + 4, :] for h in range(16)], axis=1)
    part = inner_last(head_out.astype(BF16), weight_ref[...])
    own = own_ref[...].astype(F32)
    lane = lanes((4, 128))
    token = jnp.where(lane // 32 == 2 + tp_ref[0], jnp.concatenate([own] * 4, axis=1), 0.0)
    out_ref[...] = jnp.where(lane < 64, jnp.concatenate([part, part], axis=1), token).astype(BF16)


def mlp_kernel(
    at_ref, pieces_ref, gain_ref, gate_ref, up_ref, down_ref, out_ref, tile_ref, row_ref
):
    lane = lanes((4, 128))
    blocks = []
    for kv in range(64):
        s = pieces_ref[2 * kv].astype(F32) + pieces_ref[2 * kv + 1].astype(F32)
        blocks.append(s + pltpu.roll(s, 64, 1))
    tiles = [jnp.where(lane < 64, blocks[2 * v], blocks[2 * v + 1]) for v in range(32)]
    stream = jnp.concatenate(tiles, axis=1)
    square = jnp.sum(stream * stream, axis=1, keepdims=True) * (1.0 / 4096)
    normed = (stream * lax.rsqrt(square + EPS) * gain_ref[...]).astype(BF16)
    gate = inner_last(normed, gate_ref[...])
    up = inner_last(normed, up_ref[...])
    hidden = (gate / (1.0 + jnp.exp(-gate)) * up).astype(BF16)
    down = jnp.dot(hidden, down_ref[...], preferred_element_type=F32)
    down = down + jnp.where(lanes((4, 4096)) // 32 == at_ref[0], stream, 0.0)
    for v in range(32):
        tile_ref[4 * v : 4 * v + 4, :] = down[:, 128 * v : 128 * v + 128]
    by_row = [tile_ref[pl.ds(r, 32, stride=4), :] for r in range(4)]
    wide = lanes((32, 128)) // 32
    for g in range(4):
        line = by_row[g]
        for r in range(4):
            if r != g:
                line = jnp.where(wide == r, pltpu.roll(by_row[r], (r - g) % 4 * 32, 1), line)
        row_ref[pl.ds(g, 32, stride=4), :] = line
    out_ref[...] = row_ref[...]


def total_kernel(parts_ref, out_ref):
    line = jnp.sum(parts_ref[...], axis=0, keepdims=True)
    out_ref[...] = jnp.concatenate(
        [line[:, 32 * r : 32 * r + 32] for r in range(4)], axis=0
    ).astype(BF16)


def call(kernel, name, shape, dtype, *args, scalars=0, scratch=()):
    smem = pl.BlockSpec(memory_space=pltpu.SMEM)
    vmem = pl.BlockSpec(memory_space=pltpu.VMEM)
    return pl.pallas_call(
        kernel,
        name=name,
        out_shape=SHAPE(shape, dtype),
        in_specs=[smem] * scalars + [vmem] * (len(args) - scalars),
        out_specs=vmem,
        scratch_shapes=list(scratch),
    )(*args)


def turn_tables(position):
    half_len = 32
    inv_freq = 1.0 / THETA ** (jnp.arange(half_len, dtype=F32) / half_len)
    angles = position * inv_freq
    cos_table = jnp.cos(angles)
    sin_table = jnp.sin(angles)
    cos = jnp.concatenate([cos_table] * 4)
    sin = jnp.concatenate([-sin_table, sin_table] * 2)
    return cos.reshape(1, 128), sin.reshape(1, 128)


def shards(
    tokens,
    attn_gain,
    query_weight,
    key_cache,
    value_cache,
    head_lambda,
    head_gain,
    out_weight,
    mlp_gain,
    gate_weight,
    up_weight,
    down_weight,
):
    tp = lax.axis_index("tp").astype(jnp.int32).reshape(1)
    kv = lax.axis_index(KV)
    at = lax.axis_index(KV_TP).astype(jnp.int32).reshape(1)
    other = lax.ppermute(tokens, "tp", [(0, 1), (1, 0)])
    gain = lax.dynamic_slice_in_dim(attn_gain, kv * 64, 64).reshape(1, 64)
    position = jnp.float32(key_cache.shape[1] * lax.axis_size(KV))
    cos, sin = turn_tables(position)
    lam = jnp.broadcast_to(jnp.repeat(head_lambda, 4)[:, None], (64, 128))

    part = call(
        query_kernel, "query", (72, 128), F32, tp, tokens, other, gain, query_weight, scalars=1
    )
    part = jnp.sum(shared(part, "kv_0"), axis=0)
    parts = shared(part, "kv_1")
    keys = key_cache.reshape(4, 256, 128)
    values = value_cache.reshape(4, 256, 128)
    packed = call(attend_kernel, "attend", (144, 128), BF16, parts, cos, sin, keys, values)
    packed = call(merge_kernel, "merge", (144, 128), BF16, shared(packed, "kv_0"))
    block = call(
        project_kernel,
        "project",
        (4, 128),
        BF16,
        tp,
        shared(packed, "kv_1"),
        lam,
        head_gain.reshape(1, 128),
        out_weight,
        tokens,
        scalars=1,
        scratch=[pltpu.VMEM((64, 128), F32)],
    )
    pieces = shared(block, KV_TP)
    partial = call(
        mlp_kernel,
        "mlp",
        (128, 128),
        F32,
        at,
        pieces,
        mlp_gain.reshape(1, 4096),
        gate_weight,
        up_weight,
        down_weight,
        scalars=1,
        scratch=[pltpu.VMEM((128, 128), F32), pltpu.VMEM((128, 128), F32)],
    )
    sums = lax.all_to_all(partial.reshape(128, 1, 128), KV_TP, 0, 0, tiled=True)
    return call(total_kernel, "total", (4, 32), BF16, sums.reshape(128, 128))


def solution(mesh):
    torus = Mesh(
        mesh.devices.reshape(mesh.shape["dp"], 8, 8, mesh.shape["tp"]), ("dp", "kv_0", "kv_1", "tp")
    )
    in_specs = (
        P("dp", KV_TP),
        P(),
        P(KV, "tp"),
        P("dp", KV, "tp", None),
        P("dp", KV, "tp", None),
        P("tp"),
        P(),
        P(KV, "tp"),
        P(),
        P(KV_TP, None),
        P(KV_TP, None),
        P(KV_TP, None),
    )
    out_specs = P("dp", KV_TP)
    return jax.shard_map(
        shards, mesh=torus, in_specs=in_specs, out_specs=out_specs, check_vma=False
    )
```

```python
import jax
import jax.numpy as jnp
import numpy as np
from jax import lax
from jax.experimental import pallas as pl
from jax.experimental.pallas import tpu as pltpu
from jax.sharding import Mesh
from jax.sharding import PartitionSpec as P

KV = ("kv_0", "kv_1")
KV_TP = ("kv_0", "kv_1", "tp")
EPS = 1e-06
THETA = 10000.0
F32 = jnp.float32
BF16 = jnp.bfloat16
SHAPE = jax.ShapeDtypeStruct


def lanes(shape):
    return lax.broadcasted_iota(jnp.int32, shape, len(shape) - 1)


def rows(shape):
    return lax.broadcasted_iota(jnp.int32, shape, len(shape) - 2)


def inner_last(left, right):
    return lax.dot_general(left, right, (((1,), (1,)), ((), ())), preferred_element_type=F32)


def shared(block, axis):
    copies = jnp.broadcast_to(block, (lax.axis_size(axis), *block.shape))
    return lax.all_to_all(copies, axis, 0, 0, tiled=True)


def query_kernel(tp_ref, own_ref, other_ref, gain_ref, weight_ref, out_ref):
    own = own_ref[...].astype(F32)
    other = other_ref[...].astype(F32)
    both = jnp.concatenate([own, other, own, other], axis=1)
    x = jnp.where(tp_ref[0] == 0, both[:, :64], both[:, 32:96])
    square = jnp.sum(x * x, axis=1, keepdims=True)
    scaled = (x * gain_ref[...]).astype(BF16)
    q = jnp.dot(scaled, weight_ref[...], preferred_element_type=F32)
    for h in range(16):
        out_ref[4 * h : 4 * h + 4, :] = q[:, 128 * h : 128 * h + 128]
    wide = jnp.broadcast_to(square, (4, 128))
    out_ref[64:68, :] = wide
    out_ref[68:72, :] = wide


def pack(values, lse):
    high = lse.astype(BF16).astype(F32)
    mid = (lse - high).astype(BF16).astype(F32)
    low = lse - high - mid
    at = rows((16, 128))
    tail = jnp.where(at == 0, high, jnp.where(at == 1, mid, jnp.where(at == 2, low, 0.0)))
    return values.astype(BF16), tail.astype(BF16)


def attend_kernel(parts_ref, cos_ref, sin_ref, key_ref, value_ref, out_ref):
    total = parts_ref[0]
    for k in range(1, 8):
        total = total + parts_ref[k]
    scale = lax.rsqrt(total[64:72] * (1.0 / 4096) + EPS)
    q = (total[:64].reshape(8, 8, 128) * scale[None]).reshape(64, 128)
    lane = lanes((64, 128))
    swapped = jnp.where(lane % 64 < 32, pltpu.roll(q, 96, 1), pltpu.roll(q, 32, 1))
    turned = q * cos_ref[...] + swapped * sin_ref[...]
    both = jnp.concatenate(
        [jnp.where(lane < 64, turned, 0.0), jnp.where(lane < 64, 0.0, turned)], axis=0
    ).astype(BF16)
    row = rows((128, 256)) % 4
    scores = inner_last(both, key_ref[0])
    for b in range(1, 4):
        scores = jnp.where(row == b, inner_last(both, key_ref[b]), scores)
    scores = scores * 0.125
    peak = jnp.max(scores, axis=1, keepdims=True)
    e = jnp.exp(scores - peak)
    total_e = jnp.sum(e, axis=1, keepdims=True)
    probs = e.astype(BF16)
    row_v = rows((128, 128)) % 4
    value = jnp.dot(probs, value_ref[0], preferred_element_type=F32)
    for b in range(1, 4):
        value = jnp.where(
            row_v == b, jnp.dot(probs, value_ref[b], preferred_element_type=F32), value
        )
    value = value / total_e
    lse = peak + jnp.log(total_e)
    eye = rows((128, 128)) == lanes((128, 128))
    lse_row = jnp.sum(jnp.where(eye, lse, 0.0), axis=0, keepdims=True)
    out_ref[:128, :], out_ref[128:, :] = pack(value, lse_row)


def merged(parts_ref):
    tails = []
    for k in range(8):
        tail = parts_ref[k, 128:, :].astype(F32)
        tails.append(tail[0:1] + tail[1:2] + tail[2:3])
    lse = jnp.concatenate(tails, axis=0)
    peak = jnp.max(lse, axis=0, keepdims=True)
    e = jnp.exp(lse - peak)
    total = jnp.sum(e, axis=0, keepdims=True)
    share = (e / total).T
    value = share[:, 0:1] * parts_ref[0, :128, :].astype(F32)
    for k in range(1, 8):
        value = value + share[:, k : k + 1] * parts_ref[k, :128, :].astype(F32)
    return value, peak + jnp.log(total)


def merge_kernel(parts_ref, out_ref):
    out_ref[:128, :], out_ref[128:, :] = pack(*merged(parts_ref))


def project_kernel(tp_ref, parts_ref, lam_ref, gain_ref, weight_ref, own_ref, out_ref, heads_ref):
    value, _ = merged(parts_ref)
    difference = value[:64] - lam_ref[...] * value[64:]
    norm = lax.rsqrt(jnp.mean(difference * difference, axis=1, keepdims=True) + EPS)
    heads_ref[...] = difference * norm * gain_ref[...]
    head_out = jnp.concatenate([heads_ref[4 * h : 4 * h + 4, :] for h in range(16)], axis=1)
    part = inner_last(head_out.astype(BF16), weight_ref[...])
    own = own_ref[...].astype(F32)
    lane = lanes((4, 128))
    token = jnp.where(lane // 32 == 2 + tp_ref[0], jnp.concatenate([own] * 4, axis=1), 0.0)
    out_ref[...] = jnp.where(lane < 64, jnp.concatenate([part, part], axis=1), token).astype(BF16)


def mlp_kernel(
    at_ref, pieces_ref, gain_ref, gate_ref, up_ref, down_ref, out_ref, tile_ref, row_ref
):
    lane = lanes((4, 128))
    blocks = []
    for kv in range(64):
        s = pieces_ref[2 * kv].astype(F32) + pieces_ref[2 * kv + 1].astype(F32)
        blocks.append(s + pltpu.roll(s, 64, 1))
    tiles = [jnp.where(lane < 64, blocks[2 * v], blocks[2 * v + 1]) for v in range(32)]
    stream = jnp.concatenate(tiles, axis=1)
    square = jnp.sum(stream * stream, axis=1, keepdims=True) * (1.0 / 4096)
    normed = (stream * lax.rsqrt(square + EPS) * gain_ref[...]).astype(BF16)
    gate = inner_last(normed, gate_ref[...])
    up = inner_last(normed, up_ref[...])
    hidden = (gate / (1.0 + jnp.exp(-gate)) * up).astype(BF16)
    down = jnp.dot(hidden, down_ref[...], preferred_element_type=F32)
    down = down + jnp.where(lanes((4, 4096)) // 32 == at_ref[0], stream, 0.0)
    for v in range(32):
        tile_ref[4 * v : 4 * v + 4, :] = down[:, 128 * v : 128 * v + 128]
    by_row = [tile_ref[pl.ds(r, 32, stride=4), :] for r in range(4)]
    wide = lanes((32, 128)) // 32
    for g in range(4):
        line = by_row[g]
        for r in range(4):
            if r != g:
                line = jnp.where(wide == r, pltpu.roll(by_row[r], (r - g) % 4 * 32, 1), line)
        row_ref[pl.ds(g, 32, stride=4), :] = line
    out_ref[...] = row_ref[...]


def total_kernel(parts_ref, out_ref):
    line = jnp.sum(parts_ref[...], axis=0, keepdims=True)
    out_ref[...] = jnp.concatenate(
        [line[:, 32 * r : 32 * r + 32] for r in range(4)], axis=0
    ).astype(BF16)


def call(kernel, name, shape, dtype, *args, scalars=0, scratch=()):
    smem = pl.BlockSpec(memory_space=pltpu.SMEM)
    vmem = pl.BlockSpec(memory_space=pltpu.VMEM)
    near = [pltpu.with_memory_space_constraint(x, pltpu.VMEM) for x in args[scalars:]]
    return pl.pallas_call(
        kernel,
        name=name,
        out_shape=pltpu.VMEM(shape, dtype) if name != "total" else SHAPE(shape, dtype),
        in_specs=[smem] * scalars + [vmem] * len(near),
        out_specs=vmem,
        scratch_shapes=list(scratch),
    )(*args[:scalars], *near)


def turn_tables(position):
    power = np.power(THETA, np.arange(32, dtype=np.float64) / 32).astype(np.float32)
    angles = (np.float32(position) * (np.float32(1.0) / power)).astype(np.float64)
    cos = np.tile(np.cos(angles), 4).astype(np.float32)
    sin = np.tile(np.concatenate([-np.sin(angles), np.sin(angles)]), 2).astype(np.float32)
    return jnp.asarray(cos.reshape(1, 128)), jnp.asarray(sin.reshape(1, 128))


def shards(
    tokens,
    attn_gain,
    query_weight,
    key_cache,
    value_cache,
    head_lambda,
    head_gain,
    out_weight,
    mlp_gain,
    gate_weight,
    up_weight,
    down_weight,
):
    tp = lax.axis_index("tp").astype(jnp.int32).reshape(1)
    kv = lax.axis_index(KV)
    at = lax.axis_index(KV_TP).astype(jnp.int32).reshape(1)
    other = lax.ppermute(tokens, "tp", [(0, 1), (1, 0)])
    gain = lax.dynamic_slice_in_dim(attn_gain, kv * 64, 64).reshape(1, 64)
    cos, sin = turn_tables(key_cache.shape[1] * lax.axis_size(KV))
    lam = jnp.broadcast_to(jnp.repeat(head_lambda, 4)[:, None], (64, 128))

    part = call(
        query_kernel, "query", (72, 128), F32, tp, tokens, other, gain, query_weight, scalars=1
    )
    part, cos, sin, lam, at = lax.optimization_barrier((part, cos, sin, lam, at))
    part = jnp.sum(shared(part, "kv_0"), axis=0)
    parts = shared(part, "kv_1")
    keys = key_cache.reshape(4, 256, 128)
    values = value_cache.reshape(4, 256, 128)
    packed = call(attend_kernel, "attend", (144, 128), BF16, parts, cos, sin, keys, values)
    packed = call(merge_kernel, "merge", (144, 128), BF16, shared(packed, "kv_0"))
    block = call(
        project_kernel,
        "project",
        (4, 128),
        BF16,
        tp,
        shared(packed, "kv_1"),
        lam,
        head_gain.reshape(1, 128),
        out_weight,
        tokens,
        scalars=1,
        scratch=[pltpu.VMEM((64, 128), F32)],
    )
    pieces = shared(block, KV_TP)
    partial = call(
        mlp_kernel,
        "mlp",
        (128, 128),
        F32,
        at,
        pieces,
        mlp_gain.reshape(1, 4096),
        gate_weight,
        up_weight,
        down_weight,
        scalars=1,
        scratch=[pltpu.VMEM((128, 128), F32), pltpu.VMEM((128, 128), F32)],
    )
    sums = lax.all_to_all(partial.reshape(128, 1, 128), KV_TP, 0, 0, tiled=True)
    return call(total_kernel, "total", (4, 32), BF16, sums.reshape(128, 128))


def solution(mesh):
    torus = Mesh(
        mesh.devices.reshape(mesh.shape["dp"], 8, 8, mesh.shape["tp"]), ("dp", "kv_0", "kv_1", "tp")
    )
    in_specs = (
        P("dp", KV_TP),
        P(),
        P(KV, "tp"),
        P("dp", KV, "tp", None),
        P("dp", KV, "tp", None),
        P("tp"),
        P(),
        P(KV, "tp"),
        P(),
        P(KV_TP, None),
        P(KV_TP, None),
        P(KV_TP, None),
    )
    out_specs = P("dp", KV_TP)
    return jax.shard_map(
        shards, mesh=torus, in_specs=in_specs, out_specs=out_specs, check_vma=False
    )
```

```python
import jax
import jax.numpy as jnp
import numpy as np
from jax import lax
from jax.experimental import pallas as pl
from jax.experimental.pallas import tpu as pltpu
from jax.sharding import Mesh
from jax.sharding import PartitionSpec as P

KV = ("kv_0", "kv_1")
KV_TP = ("kv_0", "kv_1", "tp")
EPS = 1e-06
THETA = 10000.0
F32 = jnp.float32
BF16 = jnp.bfloat16
SHAPE = jax.ShapeDtypeStruct


def lanes(shape):
    return lax.broadcasted_iota(jnp.int32, shape, len(shape) - 1)


def rows(shape):
    return lax.broadcasted_iota(jnp.int32, shape, len(shape) - 2)


def inner_last(left, right):
    return lax.dot_general(left, right, (((1,), (1,)), ((), ())), preferred_element_type=F32)


def shared(block, axis):
    copies = jnp.broadcast_to(block, (lax.axis_size(axis), *block.shape))
    return lax.all_to_all(copies, axis, 0, 0, tiled=True)


def prepare_kernel(
    kv_ref, own_in, weight_in, gain_in, lam_in, turn_in, head_in,
    own_ref, weight_ref, gain_ref, lam_ref, turn_ref, head_ref, all_ref, row_ref, sems,
):
    pairs = [
        (weight_in, weight_ref), (own_in, own_ref), (gain_in, all_ref), (lam_in, row_ref),
        (turn_in, turn_ref), (head_in, head_ref),
    ]
    copies = [pltpu.make_async_copy(a, b, sems.at[k]) for k, (a, b) in enumerate(pairs)]
    for copy in copies:
        copy.start()
    for copy in copies[1:]:
        copy.wait()
    line = all_ref[pl.ds(kv_ref[0] // 2, 1), :]
    gain_ref[...] = jnp.where(kv_ref[0] % 2 == 0, line, pltpu.roll(line, 64, 1))
    picked = jnp.where(lanes((64, 16)) == rows((64, 16)) // 4, row_ref[...], 0.0)
    lam_ref[...] = jnp.broadcast_to(jnp.sum(picked, axis=1, keepdims=True), (64, 128))
    copies[0].wait()


def query_kernel(tp_ref, own_ref, other_ref, gain_ref, weight_ref, out_ref):
    own = own_ref[...].astype(F32)
    other = other_ref[...].astype(F32)
    both = jnp.concatenate([own, other, own, other], axis=1)
    x = jnp.where(tp_ref[0] == 0, both[:, :64], both[:, 32:96])
    square = jnp.sum(x * x, axis=1, keepdims=True)
    scaled = (x * gain_ref[:, :64]).astype(BF16)
    q = jnp.dot(scaled, weight_ref[...], preferred_element_type=F32)
    for h in range(16):
        out_ref[4 * h : 4 * h + 4, :] = q[:, 128 * h : 128 * h + 128]
    wide = jnp.broadcast_to(square, (4, 128))
    out_ref[64:68, :] = wide
    out_ref[68:72, :] = wide


def pack(values, lse):
    high = lse.astype(BF16).astype(F32)
    mid = (lse - high).astype(BF16).astype(F32)
    low = lse - high - mid
    at = rows((16, 128))
    tail = jnp.where(at == 0, high, jnp.where(at == 1, mid, jnp.where(at == 2, low, 0.0)))
    return values.astype(BF16), tail.astype(BF16)


def attend_kernel(parts_ref, turn_ref, key_ref, value_ref, out_ref):
    total = parts_ref[0]
    for k in range(1, 8):
        total = total + parts_ref[k]
    scale = lax.rsqrt(total[64:72] * (1.0 / 4096) + EPS)
    q = (total[:64].reshape(8, 8, 128) * scale[None]).reshape(64, 128)
    lane = lanes((64, 128))
    swapped = jnp.where(lane % 64 < 32, pltpu.roll(q, 96, 1), pltpu.roll(q, 32, 1))
    turned = q * turn_ref[0:1] + swapped * turn_ref[1:2]
    both = jnp.concatenate(
        [jnp.where(lane < 64, turned, 0.0), jnp.where(lane < 64, 0.0, turned)], axis=0
    ).astype(BF16)
    row = rows((128, 256)) % 4
    scores = inner_last(both, key_ref[0])
    for b in range(1, 4):
        scores = jnp.where(row == b, inner_last(both, key_ref[b]), scores)
    scores = scores * 0.125
    peak = jnp.max(scores, axis=1, keepdims=True)
    e = jnp.exp(scores - peak)
    total_e = jnp.sum(e, axis=1, keepdims=True)
    probs = e.astype(BF16)
    row_v = rows((128, 128)) % 4
    value = jnp.dot(probs, value_ref[0], preferred_element_type=F32)
    for b in range(1, 4):
        value = jnp.where(
            row_v == b, jnp.dot(probs, value_ref[b], preferred_element_type=F32), value
        )
    value = value / total_e
    lse = peak + jnp.log(total_e)
    eye = rows((128, 128)) == lanes((128, 128))
    lse_row = jnp.sum(jnp.where(eye, lse, 0.0), axis=0, keepdims=True)
    out_ref[:128, :], out_ref[128:, :] = pack(value, lse_row)


def merged(parts_ref):
    tails = []
    for k in range(8):
        tail = parts_ref[k, 128:, :].astype(F32)
        tails.append(tail[0:1] + tail[1:2] + tail[2:3])
    lse = jnp.concatenate(tails, axis=0)
    peak = jnp.max(lse, axis=0, keepdims=True)
    e = jnp.exp(lse - peak)
    total = jnp.sum(e, axis=0, keepdims=True)
    share = (e / total).T
    value = share[:, 0:1] * parts_ref[0, :128, :].astype(F32)
    for k in range(1, 8):
        value = value + share[:, k : k + 1] * parts_ref[k, :128, :].astype(F32)
    return value, peak + jnp.log(total)


def merge_kernel(parts_ref, out_ref):
    out_ref[:128, :], out_ref[128:, :] = pack(*merged(parts_ref))


def project_kernel(tp_ref, parts_ref, lam_ref, gain_ref, weight_ref, own_ref, out_ref, heads_ref):
    value, _ = merged(parts_ref)
    difference = value[:64] - lam_ref[...] * value[64:]
    norm = lax.rsqrt(jnp.mean(difference * difference, axis=1, keepdims=True) + EPS)
    heads_ref[...] = difference * norm * gain_ref[...]
    head_out = jnp.concatenate([heads_ref[4 * h : 4 * h + 4, :] for h in range(16)], axis=1)
    part = inner_last(head_out.astype(BF16), weight_ref[...])
    part = part.astype(BF16).astype(F32)
    lane = lanes((4, 64))
    own = own_ref[...].astype(F32)
    part = part + jnp.where(lane // 32 == tp_ref[0], jnp.concatenate([own, own], axis=1), 0.0)
    out_ref[...] = jnp.concatenate([part[0:2], part[2:4]], axis=1).astype(BF16)


def mlp_kernel(
    at_ref, pieces_ref, gain_ref, gate_ref, up_ref, down_ref, out_ref, tile_ref, row_ref
):
    y = pieces_ref[...].astype(F32).reshape(32, 8, 128)
    lane = lanes((32, 8, 128))
    s = y + pltpu.roll(y, 6, 1)
    far = pltpu.roll(s, 4, 1)
    front = jnp.where(lane < 64, s, pltpu.roll(far, 64, 2))
    back = jnp.where(lane < 64, pltpu.roll(s, 64, 2), far)
    four = jnp.where(rows((32, 8, 128)) < 2, front, pltpu.roll(back, 2, 1))
    stream = jnp.concatenate([four[v, 0:4] for v in range(32)], axis=1)
    square = jnp.sum(stream * stream, axis=1, keepdims=True) * (1.0 / 4096)
    normed = (stream * lax.rsqrt(square + EPS) * gain_ref[...]).astype(BF16)
    gate = inner_last(normed, gate_ref[...])
    up = inner_last(normed, up_ref[...])
    hidden = (gate / (1.0 + jnp.exp(-gate)) * up).astype(BF16)
    down = jnp.dot(hidden, down_ref[...], preferred_element_type=F32)
    down = down + jnp.where(lanes((4, 4096)) // 32 == at_ref[0], stream, 0.0)
    for v in range(32):
        tile_ref[4 * v : 4 * v + 4, :] = down[:, 128 * v : 128 * v + 128]
    by_row = [tile_ref[pl.ds(r, 32, stride=4), :] for r in range(4)]
    wide = lanes((32, 128)) // 32
    for g in range(4):
        line = by_row[g]
        for r in range(4):
            if r != g:
                line = jnp.where(wide == r, pltpu.roll(by_row[r], (r - g) % 4 * 32, 1), line)
        row_ref[pl.ds(g, 32, stride=4), :] = line
    out_ref[...] = row_ref[...]


def total_kernel(parts_ref, out_ref):
    line = jnp.sum(parts_ref[...], axis=0, keepdims=True)
    out_ref[...] = jnp.concatenate(
        [line[:, 32 * r : 32 * r + 32] for r in range(4)], axis=0
    ).astype(BF16)


def call(kernel, name, shape, dtype, *args, scalars=0, scratch=()):
    smem = pl.BlockSpec(memory_space=pltpu.SMEM)
    vmem = pl.BlockSpec(memory_space=pltpu.VMEM)
    near = [pltpu.with_memory_space_constraint(x, pltpu.VMEM) for x in args[scalars:]]
    return pl.pallas_call(
        kernel,
        name=name,
        out_shape=pltpu.VMEM(shape, dtype) if name != "total" else SHAPE(shape, dtype),
        in_specs=[smem] * scalars + [vmem] * len(near),
        out_specs=vmem,
        scratch_shapes=list(scratch),
    )(*args[:scalars], *near)


def turn_tables(position):
    inverse = np.power(THETA, -np.arange(32, dtype=np.float64) / 32).astype(np.float32)
    angles = (np.float32(position) * inverse).astype(np.float64)
    cos = np.tile(np.cos(angles), 4)
    sin = np.tile(np.concatenate([-np.sin(angles), np.sin(angles)]), 2)
    return jnp.asarray(np.stack([cos, sin] + [np.zeros(128)] * 6).astype(np.float32))


def shards(
    tokens,
    attn_gain,
    query_weight,
    key_cache,
    value_cache,
    head_lambda,
    head_gain,
    out_weight,
    mlp_gain,
    gate_weight,
    up_weight,
    down_weight,
):
    tp = lax.axis_index("tp").astype(jnp.int32).reshape(1)
    kv = lax.axis_index(KV)
    at = lax.axis_index(KV_TP).astype(jnp.int32).reshape(1)
    other = lax.ppermute(tokens, "tp", [(0, 1), (1, 0)])
    turn = turn_tables(key_cache.shape[1] * lax.axis_size(KV))
    own, weight, gain, lam, turn, head = pl.pallas_call(
        prepare_kernel,
        name="prepare",
        out_shape=[
            pltpu.VMEM((4, 32), BF16),
            pltpu.VMEM((64, 2048), BF16),
            pltpu.VMEM((1, 128), F32),
            pltpu.VMEM((64, 128), F32),
            pltpu.VMEM((8, 128), F32),
            pltpu.VMEM((1, 128), F32),
        ],
        in_specs=[pl.BlockSpec(memory_space=pltpu.SMEM)] + [pl.BlockSpec(memory_space=pl.ANY)] * 6,
        out_specs=[pl.BlockSpec(memory_space=pltpu.VMEM)] * 6,
        scratch_shapes=[
            pltpu.VMEM((32, 128), F32),
            pltpu.VMEM((1, 16), F32),
            pltpu.SemaphoreType.DMA((6,)),
        ],
    )(
        kv.astype(jnp.int32).reshape(1),
        tokens,
        query_weight,
        attn_gain.reshape(32, 128),
        head_lambda.reshape(1, 16),
        turn,
        head_gain.reshape(1, 128),
    )
    part = call(query_kernel, "query", (72, 128), F32, tp, own, other, gain, weight, scalars=1)
    part, at = lax.optimization_barrier((part, at))
    part = jnp.sum(shared(part, "kv_0"), axis=0)
    parts = shared(part, "kv_1")
    keys = key_cache.reshape(4, 256, 128)
    values = value_cache.reshape(4, 256, 128)
    packed = call(attend_kernel, "attend", (144, 128), BF16, parts, turn, keys, values)
    packed = call(merge_kernel, "merge", (144, 128), BF16, shared(packed, "kv_0"))
    block = call(
        project_kernel,
        "project",
        (2, 128),
        BF16,
        tp,
        shared(packed, "kv_1"),
        lam,
        head,
        out_weight,
        own,
        scalars=1,
        scratch=[pltpu.VMEM((64, 128), F32)],
    )
    pieces = shared(block, KV_TP).reshape(256, 128)
    partial = call(
        mlp_kernel,
        "mlp",
        (128, 128),
        F32,
        at,
        pieces,
        mlp_gain.reshape(1, 4096),
        gate_weight,
        up_weight,
        down_weight,
        scalars=1,
        scratch=[pltpu.VMEM((128, 128), F32), pltpu.VMEM((128, 128), F32)],
    )
    sums = lax.all_to_all(partial.reshape(128, 1, 128), KV_TP, 0, 0, tiled=True)
    return call(total_kernel, "total", (4, 32), BF16, sums.reshape(128, 128))


def solution(mesh):
    torus = Mesh(
        mesh.devices.reshape(mesh.shape["dp"], 8, 8, mesh.shape["tp"]), ("dp", "kv_0", "kv_1", "tp")
    )
    in_specs = (
        P("dp", KV_TP),
        P(),
        P(KV, "tp"),
        P("dp", KV, "tp", None),
        P("dp", KV, "tp", None),
        P("tp"),
        P(),
        P(KV, "tp"),
        P(),
        P(KV_TP, None),
        P(KV_TP, None),
        P(KV_TP, None),
    )
    out_specs = P("dp", KV_TP)
    return jax.shard_map(
        shards, mesh=torus, in_specs=in_specs, out_specs=out_specs, check_vma=False
    )
```

```python
import jax
import jax.numpy as jnp
import numpy as np
from jax import lax
from jax.experimental import pallas as pl
from jax.experimental.pallas import tpu as pltpu
from jax.sharding import Mesh
from jax.sharding import PartitionSpec as P

KV = ("kv_0", "kv_1")
KV_TP = ("kv_0", "kv_1", "tp")
EPS = 1e-06
THETA = 10000.0
F32 = jnp.float32
BF16 = jnp.bfloat16
SHAPE = jax.ShapeDtypeStruct


def lanes(shape):
    return lax.broadcasted_iota(jnp.int32, shape, len(shape) - 1)


def rows(shape):
    return lax.broadcasted_iota(jnp.int32, shape, len(shape) - 2)


def inner_last(left, right):
    return lax.dot_general(left, right, (((1,), (1,)), ((), ())), preferred_element_type=F32)


def shared(block, axis):
    copies = jnp.broadcast_to(block, (lax.axis_size(axis), *block.shape))
    return lax.all_to_all(copies, axis, 0, 0, tiled=True)


def prepare_kernel(
    kv_ref, own_in, weight_in, gain_in, lam_in, turn_in, head_in, key_in, value_in,
    own_ref, weight_ref, gain_ref, lam_ref, turn_ref, head_ref, cache_ref, all_ref, row_ref, sems,
):
    away = pl.ds(2 - 2 * (kv_ref[0] // 8 % 2), 2)
    pairs = [
        (weight_in, weight_ref), (key_in.at[away], cache_ref.at[0:2]),
        (value_in.at[away], cache_ref.at[2:4]), (own_in, own_ref), (gain_in, all_ref),
        (lam_in, row_ref), (turn_in, turn_ref), (head_in, head_ref),
    ]
    copies = [pltpu.make_async_copy(a, b, sems.at[k]) for k, (a, b) in enumerate(pairs)]
    for copy in copies:
        copy.start()
    for copy in copies[3:]:
        copy.wait()
    line = all_ref[pl.ds(kv_ref[0] // 2, 1), :]
    gain_ref[...] = jnp.where(kv_ref[0] % 2 == 0, line, pltpu.roll(line, 64, 1))
    picked = jnp.where(lanes((32, 16)) == rows((32, 16)) // 2, row_ref[...], 0.0)
    lam_ref[...] = jnp.broadcast_to(jnp.sum(picked, axis=1, keepdims=True), (32, 128))
    for copy in copies[:3]:
        copy.wait()


def query_kernel(tp_ref, own_ref, other_ref, gain_ref, weight_ref, out_ref):
    own = own_ref[...].astype(F32)
    other = other_ref[...].astype(F32)
    both = jnp.concatenate([own, other, own, other], axis=1)
    x = jnp.where(tp_ref[0] == 0, both[:, :64], both[:, 32:96])
    square = jnp.sum(x * x, axis=1, keepdims=True)
    scaled = (x * gain_ref[:, :64]).astype(BF16)
    q = jnp.dot(scaled, weight_ref[...], preferred_element_type=F32)
    wide = jnp.broadcast_to(square, (4, 128))
    for pair in range(2):
        two = slice(2 * pair, 2 * pair + 2)
        for h in range(16):
            out_ref[pair, 2 * h : 2 * h + 2, :] = q[two, 128 * h : 128 * h + 128]
        for k in range(4):
            out_ref[pair, 32 + 2 * k : 34 + 2 * k, :] = wide[two]


def pack(values, lse):
    high = lse.astype(BF16).astype(F32)
    mid = (lse - high).astype(BF16).astype(F32)
    low = lse - high - mid
    at = rows((16, 128))
    tail = jnp.where(at == 0, high, jnp.where(at == 1, mid, jnp.where(at == 2, low, 0.0)))
    return values.astype(BF16), tail.astype(BF16)


def attend_kernel(pair_ref, part_ref, turn_ref, key_ref, value_ref, cache_ref, out_ref):
    total = part_ref[...]
    scale = lax.rsqrt(total[32:40] * (1.0 / 4096) + EPS)
    q = (total[:32].reshape(4, 8, 128) * scale[None]).reshape(32, 128)
    lane = lanes((32, 128))
    swapped = jnp.where(lane % 64 < 32, pltpu.roll(q, 96, 1), pltpu.roll(q, 32, 1))
    turned = q * turn_ref[0:1] + swapped * turn_ref[1:2]
    both = jnp.concatenate(
        [jnp.where(lane < 64, turned, 0.0), jnp.where(lane < 64, 0.0, turned)], axis=0
    ).astype(BF16)
    here = 2 * pair_ref[0]

    def against(b):
        near = inner_last(both, key_ref[here + b])
        return jnp.concatenate([near, inner_last(both, cache_ref[b])], axis=1)

    scores = jnp.where(rows((64, 512)) % 2 == 0, against(0), against(1)) * 0.125
    peak = jnp.max(scores, axis=1, keepdims=True)
    e = jnp.exp(scores - peak)
    total_e = jnp.sum(e, axis=1, keepdims=True)
    probs = e.astype(BF16)

    def valued(b):
        near = jnp.dot(probs[:, :256], value_ref[here + b], preferred_element_type=F32)
        return near + jnp.dot(probs[:, 256:], cache_ref[2 + b], preferred_element_type=F32)

    value = jnp.where(rows((64, 128)) % 2 == 0, valued(0), valued(1)) / total_e
    lse = peak + jnp.log(total_e)
    eye = rows((64, 128)) == lanes((64, 128))
    lse_row = jnp.sum(jnp.where(eye, lse, 0.0), axis=0, keepdims=True)
    out_ref[:64, :], out_ref[64:, :] = pack(value, lse_row)


def lse_of(parts_ref):
    tails = []
    for k in range(8):
        tail = parts_ref[k, 64:, :].astype(F32)
        tails.append(tail[0:1] + tail[1:2] + tail[2:3])
    return jnp.concatenate(tails, axis=0)


def weighed(parts_ref, share, slots):
    value = 0.0
    for k in slots:
        value = value + share[:64, k : k + 1] * parts_ref[k, :64, :].astype(F32)
    return value


def merge_kernel(parts_ref, out_ref):
    lse = lse_of(parts_ref)
    peak = jnp.max(lse, axis=0, keepdims=True)
    e = jnp.exp(lse - peak)
    total = jnp.sum(e, axis=0, keepdims=True)
    value = weighed(parts_ref, (e / total).T, range(8))
    out_ref[:64, :], out_ref[64:, :] = pack(value, peak + jnp.log(total))


def project_kernel(tp_ref, parts_ref, lam_ref, gain_ref, weight_ref, own_ref, out_ref, heads_ref):
    lse = lse_of(parts_ref)
    even = rows((8, 128)) % 2 == 0
    low = jnp.finfo(F32).min
    peak = jnp.where(
        even,
        jnp.max(jnp.where(even, lse, low), axis=0, keepdims=True),
        jnp.max(jnp.where(even, low, lse), axis=0, keepdims=True),
    )
    e = jnp.exp(lse - peak)
    total = jnp.where(
        even,
        jnp.sum(jnp.where(even, e, 0.0), axis=0, keepdims=True),
        jnp.sum(jnp.where(even, 0.0, e), axis=0, keepdims=True),
    )
    share = (e / total).T
    for pair in range(2):
        value = weighed(parts_ref, share, range(pair, 8, 2))
        difference = value[:32] - lam_ref[...] * value[32:]
        norm = lax.rsqrt(jnp.mean(difference * difference, axis=1, keepdims=True) + EPS)
        heads_ref[32 * pair : 32 * pair + 32, :] = difference * norm * gain_ref[...]
    head_out = jnp.concatenate(
        [
            jnp.concatenate(
                [heads_ref[32 * pair + 2 * h : 32 * pair + 2 * h + 2, :] for h in range(16)], axis=1
            )
            for pair in range(2)
        ],
        axis=0,
    )
    part = inner_last(head_out.astype(BF16), weight_ref[...])
    part = part.astype(BF16).astype(F32)
    lane = lanes((4, 64))
    own = own_ref[...].astype(F32)
    part = part + jnp.where(lane // 32 == tp_ref[0], jnp.concatenate([own, own], axis=1), 0.0)
    out_ref[...] = jnp.concatenate([part[0:2], part[2:4]], axis=1).astype(BF16)


def mlp_kernel(
    at_ref, pieces_ref, gain_ref, gate_ref, up_ref, down_ref, out_ref, tile_ref, row_ref
):
    y = pieces_ref[...].astype(F32).reshape(32, 8, 128)
    lane = lanes((32, 8, 128))
    s = y + pltpu.roll(y, 6, 1)
    far = pltpu.roll(s, 4, 1)
    front = jnp.where(lane < 64, s, pltpu.roll(far, 64, 2))
    back = jnp.where(lane < 64, pltpu.roll(s, 64, 2), far)
    four = jnp.where(rows((32, 8, 128)) < 2, front, pltpu.roll(back, 2, 1))
    stream = jnp.concatenate([four[v, 0:4] for v in range(32)], axis=1)
    square = jnp.sum(stream * stream, axis=1, keepdims=True) * (1.0 / 4096)
    normed = (stream * lax.rsqrt(square + EPS) * gain_ref[...]).astype(BF16)
    gate = inner_last(normed, gate_ref[...])
    up = inner_last(normed, up_ref[...])
    hidden = (gate / (1.0 + jnp.exp(-gate)) * up).astype(BF16)
    down = jnp.dot(hidden, down_ref[...], preferred_element_type=F32)
    down = down + jnp.where(lanes((4, 4096)) // 32 == at_ref[0], stream, 0.0)
    for v in range(32):
        tile_ref[4 * v : 4 * v + 4, :] = down[:, 128 * v : 128 * v + 128]
    by_row = [tile_ref[pl.ds(r, 32, stride=4), :] for r in range(4)]
    wide = lanes((32, 128)) // 32
    for g in range(4):
        line = by_row[g]
        for r in range(4):
            if r != g:
                line = jnp.where(wide == r, pltpu.roll(by_row[r], (r - g) % 4 * 32, 1), line)
        row_ref[pl.ds(g, 32, stride=4), :] = line
    out_ref[...] = row_ref[...]


def total_kernel(parts_ref, out_ref):
    line = jnp.sum(parts_ref[...], axis=0, keepdims=True)
    out_ref[...] = jnp.concatenate(
        [line[:, 32 * r : 32 * r + 32] for r in range(4)], axis=0
    ).astype(BF16)


def call(kernel, name, shape, dtype, *args, scalars=0, scratch=()):
    smem = pl.BlockSpec(memory_space=pltpu.SMEM)
    vmem = pl.BlockSpec(memory_space=pltpu.VMEM)
    near = [pltpu.with_memory_space_constraint(x, pltpu.VMEM) for x in args[scalars:]]
    return pl.pallas_call(
        kernel,
        out_shape=pltpu.VMEM(shape, dtype) if name != "total" else SHAPE(shape, dtype),
        in_specs=[smem] * scalars + [vmem] * len(near),
        out_specs=vmem,
        scratch_shapes=list(scratch),
    )(*args[:scalars], *near)


def turn_tables(position):
    inverse = np.power(THETA, -np.arange(32, dtype=np.float64) / 32).astype(np.float32)
    angles = (np.float32(position) * inverse).astype(np.float64)
    cos = np.tile(np.cos(angles), 4)
    sin = np.tile(np.concatenate([-np.sin(angles), np.sin(angles)]), 2)
    return jnp.asarray(np.stack([cos, sin] + [np.zeros(128)] * 6).astype(np.float32))


def shards(
    tokens,
    attn_gain,
    query_weight,
    key_cache,
    value_cache,
    head_lambda,
    head_gain,
    out_weight,
    mlp_gain,
    gate_weight,
    up_weight,
    down_weight,
):
    tp = lax.axis_index("tp").astype(jnp.int32).reshape(1)
    kv = lax.axis_index(KV)
    at = lax.axis_index(KV_TP).astype(jnp.int32).reshape(1)
    other = lax.ppermute(tokens, "tp", [(0, 1), (1, 0)])
    turn = turn_tables(key_cache.shape[1] * lax.axis_size(KV))
    keys = key_cache.reshape(4, 256, 128)
    values = value_cache.reshape(4, 256, 128)
    pair = (kv // 8 % 2).astype(jnp.int32).reshape(1)
    own, weight, gain, lam, turn, head, cache = pl.pallas_call(
        prepare_kernel,
        name="prepare",
        out_shape=[
            pltpu.VMEM((4, 32), BF16),
            pltpu.VMEM((64, 2048), BF16),
            pltpu.VMEM((1, 128), F32),
            pltpu.VMEM((32, 128), F32),
            pltpu.VMEM((8, 128), F32),
            pltpu.VMEM((1, 128), F32),
            pltpu.VMEM((4, 256, 128), BF16),
        ],
        in_specs=[pl.BlockSpec(memory_space=pltpu.SMEM)] + [pl.BlockSpec(memory_space=pl.ANY)] * 8,
        out_specs=[pl.BlockSpec(memory_space=pltpu.VMEM)] * 7,
        scratch_shapes=[
            pltpu.VMEM((32, 128), F32),
            pltpu.VMEM((1, 16), F32),
            pltpu.SemaphoreType.DMA((8,)),
        ],
    )(
        kv.astype(jnp.int32).reshape(1),
        tokens,
        query_weight,
        attn_gain.reshape(32, 128),
        head_lambda.reshape(1, 16),
        turn,
        head_gain.reshape(1, 128),
        keys,
        values,
    )
    part = call(query_kernel, "query", (2, 40, 128), F32, tp, own, other, gain, weight, scalars=1)
    part, at, pair = lax.optimization_barrier((part, at, pair))
    copies = jnp.broadcast_to(part[None], (4, 2, 40, 128)).reshape(8, 40, 128)
    part = jnp.sum(lax.all_to_all(copies, "kv_0", 0, 0, tiled=True), axis=0)
    part, cache = lax.optimization_barrier((part, cache))
    cache = lax.ppermute(cache, "kv_0", [(z, z ^ 1) for z in range(8)])
    parts = shared(part, "kv_1")
    part = jnp.sum(parts, axis=0)
    packed = call(
        attend_kernel,
        "attend",
        (80, 128),
        BF16,
        pair,
        part,
        turn,
        keys,
        values,
        cache,
        scalars=1,
    )
    packed = call(merge_kernel, "merge", (80, 128), BF16, shared(packed, "kv_1"))
    block = call(
        project_kernel,
        "project",
        (2, 128),
        BF16,
        tp,
        shared(packed, "kv_0"),
        lam,
        head,
        out_weight,
        own,
        scalars=1,
        scratch=[pltpu.VMEM((64, 128), F32)],
    )
    pieces = shared(block, KV_TP).reshape(256, 128)
    partial = call(
        mlp_kernel,
        "mlp",
        (128, 128),
        F32,
        at,
        pieces,
        mlp_gain.reshape(1, 4096),
        gate_weight,
        up_weight,
        down_weight,
        scalars=1,
        scratch=[pltpu.VMEM((128, 128), F32), pltpu.VMEM((128, 128), F32)],
    )
    sums = lax.all_to_all(partial.reshape(128, 1, 128), KV_TP, 0, 0, tiled=True)
    return call(total_kernel, "total", (4, 32), BF16, sums.reshape(128, 128))


def solution(mesh):
    torus = Mesh(
        mesh.devices.reshape(mesh.shape["dp"], 8, 8, mesh.shape["tp"]), ("dp", "kv_0", "kv_1", "tp")
    )
    in_specs = (
        P("dp", KV_TP),
        P(),
        P(KV, "tp"),
        P("dp", KV, "tp", None),
        P("dp", KV, "tp", None),
        P("tp"),
        P(),
        P(KV, "tp"),
        P(),
        P(KV_TP, None),
        P(KV_TP, None),
        P(KV_TP, None),
    )
    out_specs = P("dp", KV_TP)
    return jax.shard_map(
        shards, mesh=torus, in_specs=in_specs, out_specs=out_specs, check_vma=False
    )
```

```python
import jax
import jax.numpy as jnp
import numpy as np
from jax import lax
from jax.experimental import pallas as pl
from jax.experimental.pallas import tpu as pltpu
from jax.sharding import Mesh
from jax.sharding import PartitionSpec as P

KV = ("kv_0", "kv_1")
KV_TP = ("kv_0", "kv_1", "tp")
EPS = 1e-06
THETA = 10000.0
F32 = jnp.float32
BF16 = jnp.bfloat16
SHAPE = jax.ShapeDtypeStruct


def lanes(shape):
    return lax.broadcasted_iota(jnp.int32, shape, len(shape) - 1)


def rows(shape):
    return lax.broadcasted_iota(jnp.int32, shape, len(shape) - 2)


def inner_last(left, right):
    return lax.dot_general(left, right, (((1,), (1,)), ((), ())), preferred_element_type=F32)


def shared(block, axis):
    copies = jnp.broadcast_to(block, (lax.axis_size(axis), *block.shape))
    return lax.all_to_all(copies, axis, 0, 0, tiled=True)


def prepare_kernel(
    kv_ref, own_in, weight_in, gain_in, lam_in, turn_in, head_in, key_in, value_in,
    own_ref, weight_ref, gain_ref, lam_ref, turn_ref, head_ref, cache_ref, all_ref, row_ref, sems,
):
    away = pl.ds(2 - 2 * (kv_ref[0] // 8 % 2), 2)
    pairs = [
        (weight_in, weight_ref), (key_in.at[away], cache_ref.at[0:2]),
        (value_in.at[away], cache_ref.at[2:4]), (own_in, own_ref), (gain_in, all_ref),
        (lam_in, row_ref), (turn_in, turn_ref), (head_in, head_ref),
    ]
    copies = [pltpu.make_async_copy(a, b, sems.at[k]) for k, (a, b) in enumerate(pairs)]
    for copy in copies:
        copy.start()
    for copy in copies[3:]:
        copy.wait()
    line = all_ref[pl.ds(kv_ref[0] // 2, 1), :]
    gain_ref[...] = jnp.where(kv_ref[0] % 2 == 0, line, pltpu.roll(line, 64, 1))
    picked = jnp.where(lanes((32, 16)) == rows((32, 16)) // 2, row_ref[...], 0.0)
    lam_ref[...] = jnp.broadcast_to(jnp.sum(picked, axis=1, keepdims=True), (32, 128))
    for copy in copies[:3]:
        copy.wait()


def query_kernel(tp_ref, own_ref, other_ref, gain_ref, weight_ref, out_ref):
    own = own_ref[...].astype(F32)
    other = other_ref[...].astype(F32)
    both = jnp.concatenate([own, other, own, other], axis=1)
    x = jnp.where(tp_ref[0] == 0, both[:, :64], both[:, 32:96])
    square = jnp.sum(x * x, axis=1, keepdims=True)
    scaled = (x * gain_ref[:, :64]).astype(BF16)
    q = jnp.dot(scaled, weight_ref[...], preferred_element_type=F32)
    wide = jnp.broadcast_to(square, (4, 128))
    for pair in range(2):
        two = slice(2 * pair, 2 * pair + 2)
        for h in range(16):
            out_ref[pair, 2 * h : 2 * h + 2, :] = q[two, 128 * h : 128 * h + 128]
        for k in range(4):
            out_ref[pair, 32 + 2 * k : 34 + 2 * k, :] = wide[two]


def pack(values, lse):
    high = lse.astype(BF16).astype(F32)
    mid = (lse - high).astype(BF16).astype(F32)
    low = lse - high - mid
    at = rows((8, 128))
    tail = jnp.where(at == 0, high, jnp.where(at == 1, mid, jnp.where(at == 2, low, 0.0)))
    return values.astype(BF16), tail.astype(BF16)


def attend_kernel(pair_ref, part_ref, turn_ref, key_ref, value_ref, cache_ref, out_ref):
    total = part_ref[...]
    scale = lax.rsqrt(total[32:40] * (1.0 / 4096) + EPS)
    q = (total[:32].reshape(4, 8, 128) * scale[None]).reshape(32, 128)
    lane = lanes((32, 128))
    swapped = jnp.where(lane % 64 < 32, pltpu.roll(q, 96, 1), pltpu.roll(q, 32, 1))
    turned = q * turn_ref[0:1] + swapped * turn_ref[1:2]
    both = jnp.concatenate(
        [jnp.where(lane < 64, turned, 0.0), jnp.where(lane < 64, 0.0, turned)], axis=0
    ).astype(BF16)
    here = 2 * pair_ref[0]

    def against(b):
        near = inner_last(both, key_ref[here + b])
        return jnp.concatenate([near, inner_last(both, cache_ref[b])], axis=1)

    scores = jnp.where(rows((64, 512)) % 2 == 0, against(0), against(1)) * 0.125
    peak = jnp.max(scores, axis=1, keepdims=True)
    e = jnp.exp(scores - peak)
    total_e = jnp.sum(e, axis=1, keepdims=True)
    probs = e.astype(BF16)

    def valued(b):
        near = jnp.dot(probs[:, :256], value_ref[here + b], preferred_element_type=F32)
        return near + jnp.dot(probs[:, 256:], cache_ref[2 + b], preferred_element_type=F32)

    value = jnp.where(rows((64, 128)) % 2 == 0, valued(0), valued(1)) / total_e
    lse = peak + jnp.log(total_e)
    eye = rows((64, 128)) == lanes((64, 128))
    lse_row = jnp.sum(jnp.where(eye, lse, 0.0), axis=0, keepdims=True)
    out_ref[:64, :], out_ref[64:, :] = pack(value, lse_row)


def lse_of(parts_ref):
    tails = []
    for k in range(8):
        tail = parts_ref[k, 64:, :].astype(F32)
        tails.append(tail[0:1] + tail[1:2] + tail[2:3])
    return jnp.concatenate(tails, axis=0)


def weighed(parts_ref, share, slots):
    value = 0.0
    for k in slots:
        value = value + share[:64, k : k + 1] * parts_ref[k, :64, :].astype(F32)
    return value


def merge_kernel(parts_ref, out_ref):
    lse = lse_of(parts_ref)
    peak = jnp.max(lse, axis=0, keepdims=True)
    e = jnp.exp(lse - peak)
    total = jnp.sum(e, axis=0, keepdims=True)
    value = weighed(parts_ref, (e / total).T, range(8))
    out_ref[:64, :], out_ref[64:, :] = pack(value, peak + jnp.log(total))


def project_kernel(tp_ref, parts_ref, lam_ref, gain_ref, weight_ref, own_ref, out_ref, heads_ref):
    lse = lse_of(parts_ref)
    even = rows((8, 128)) % 2 == 0
    low = jnp.finfo(F32).min
    peak = jnp.where(
        even,
        jnp.max(jnp.where(even, lse, low), axis=0, keepdims=True),
        jnp.max(jnp.where(even, low, lse), axis=0, keepdims=True),
    )
    e = jnp.exp(lse - peak)
    total = jnp.where(
        even,
        jnp.sum(jnp.where(even, e, 0.0), axis=0, keepdims=True),
        jnp.sum(jnp.where(even, 0.0, e), axis=0, keepdims=True),
    )
    share = (e / total).T
    for pair in range(2):
        value = weighed(parts_ref, share, range(pair, 8, 2))
        difference = value[:32] - lam_ref[...] * value[32:]
        norm = lax.rsqrt(jnp.mean(difference * difference, axis=1, keepdims=True) + EPS)
        heads_ref[32 * pair : 32 * pair + 32, :] = difference * norm * gain_ref[...]
    head_out = jnp.concatenate(
        [
            jnp.concatenate(
                [heads_ref[32 * pair + 2 * h : 32 * pair + 2 * h + 2, :] for h in range(16)], axis=1
            )
            for pair in range(2)
        ],
        axis=0,
    )
    part = inner_last(head_out.astype(BF16), weight_ref[...])
    part = part.astype(BF16).astype(F32)
    lane = lanes((4, 64))
    own = own_ref[...].astype(F32)
    part = part + jnp.where(lane // 32 == tp_ref[0], jnp.concatenate([own, own], axis=1), 0.0)
    out_ref[...] = jnp.concatenate([part[0:2], part[2:4]], axis=1).astype(BF16)


def mlp_kernel(
    at_ref, pieces_ref, gain_ref, gate_ref, up_ref, down_ref, out_ref, tile_ref, row_ref
):
    y = pieces_ref[...].astype(F32).reshape(32, 8, 128)
    lane = lanes((32, 8, 128))
    s = y + pltpu.roll(y, 6, 1)
    far = pltpu.roll(s, 4, 1)
    front = jnp.where(lane < 64, s, pltpu.roll(far, 64, 2))
    back = jnp.where(lane < 64, pltpu.roll(s, 64, 2), far)
    four = jnp.where(rows((32, 8, 128)) < 2, front, pltpu.roll(back, 2, 1))
    stream = jnp.concatenate([four[v, 0:4] for v in range(32)], axis=1)
    square = jnp.sum(stream * stream, axis=1, keepdims=True) * (1.0 / 4096)
    normed = (stream * lax.rsqrt(square + EPS) * gain_ref[...]).astype(BF16)
    gate = inner_last(normed, gate_ref[...])
    up = inner_last(normed, up_ref[...])
    hidden = (gate / (1.0 + jnp.exp(-gate)) * up).astype(BF16)
    down = jnp.dot(hidden, down_ref[...], preferred_element_type=F32)
    down = down + jnp.where(lanes((4, 4096)) // 32 == at_ref[0], stream, 0.0)
    for v in range(32):
        tile_ref[4 * v : 4 * v + 4, :] = down[:, 128 * v : 128 * v + 128]
    by_row = [tile_ref[pl.ds(r, 32, stride=4), :] for r in range(4)]
    wide = lanes((32, 128)) // 32
    for g in range(4):
        line = by_row[g]
        for r in range(4):
            if r != g:
                line = jnp.where(wide == r, pltpu.roll(by_row[r], (r - g) % 4 * 32, 1), line)
        row_ref[pl.ds(g, 32, stride=4), :] = line
    out_ref[...] = row_ref[...]


def total_kernel(parts_ref, out_ref):
    line = jnp.sum(parts_ref[...], axis=0, keepdims=True)
    out_ref[...] = jnp.concatenate(
        [line[:, 32 * r : 32 * r + 32] for r in range(4)], axis=0
    ).astype(BF16)


def call(kernel, name, shape, dtype, *args, scalars=0, scratch=()):
    smem = pl.BlockSpec(memory_space=pltpu.SMEM)
    vmem = pl.BlockSpec(memory_space=pltpu.VMEM)
    near = [pltpu.with_memory_space_constraint(x, pltpu.VMEM) for x in args[scalars:]]
    return pl.pallas_call(
        kernel,
        out_shape=pltpu.VMEM(shape, dtype) if name != "total" else SHAPE(shape, dtype),
        in_specs=[smem] * scalars + [vmem] * len(near),
        out_specs=vmem,
        scratch_shapes=list(scratch),
    )(*args[:scalars], *near)


def turn_tables(position):
    inverse = np.power(THETA, -np.arange(32, dtype=np.float64) / 32).astype(np.float32)
    angles = (np.float32(position) * inverse).astype(np.float64)
    cos = np.tile(np.cos(angles), 4)
    sin = np.tile(np.concatenate([-np.sin(angles), np.sin(angles)]), 2)
    return jnp.asarray(np.stack([cos, sin] + [np.zeros(128)] * 6).astype(np.float32))


def shards(
    tokens,
    attn_gain,
    query_weight,
    key_cache,
    value_cache,
    head_lambda,
    head_gain,
    out_weight,
    mlp_gain,
    gate_weight,
    up_weight,
    down_weight,
):
    tp = lax.axis_index("tp").astype(jnp.int32).reshape(1)
    kv = lax.axis_index(KV)
    at = lax.axis_index(KV_TP).astype(jnp.int32).reshape(1)
    other = lax.ppermute(tokens, "tp", [(0, 1), (1, 0)])
    turn = turn_tables(key_cache.shape[1] * lax.axis_size(KV))
    keys = key_cache.reshape(4, 256, 128)
    values = value_cache.reshape(4, 256, 128)
    pair = (kv // 8 % 2).astype(jnp.int32).reshape(1)
    own, weight, gain, lam, turn, head, cache = pl.pallas_call(
        prepare_kernel,
        name="prepare",
        out_shape=[
            pltpu.VMEM((4, 32), BF16),
            pltpu.VMEM((64, 2048), BF16),
            pltpu.VMEM((1, 128), F32),
            pltpu.VMEM((32, 128), F32),
            pltpu.VMEM((8, 128), F32),
            pltpu.VMEM((1, 128), F32),
            pltpu.VMEM((4, 256, 128), BF16),
        ],
        in_specs=[pl.BlockSpec(memory_space=pltpu.SMEM)] + [pl.BlockSpec(memory_space=pl.ANY)] * 8,
        out_specs=[pl.BlockSpec(memory_space=pltpu.VMEM)] * 7,
        scratch_shapes=[
            pltpu.VMEM((32, 128), F32),
            pltpu.VMEM((1, 16), F32),
            pltpu.SemaphoreType.DMA((8,)),
        ],
    )(
        kv.astype(jnp.int32).reshape(1),
        tokens,
        query_weight,
        attn_gain.reshape(32, 128),
        head_lambda.reshape(1, 16),
        turn,
        head_gain.reshape(1, 128),
        keys,
        values,
    )
    part = call(query_kernel, "query", (2, 40, 128), F32, tp, own, other, gain, weight, scalars=1)
    part, at, pair = lax.optimization_barrier((part, at, pair))
    copies = jnp.broadcast_to(part[None], (4, 2, 40, 128)).reshape(8, 40, 128)
    part = jnp.sum(lax.all_to_all(copies, "kv_0", 0, 0, tiled=True), axis=0)
    part, cache = lax.optimization_barrier((part, cache))
    cache = lax.ppermute(cache, "kv_0", [(z, z ^ 1) for z in range(8)])
    parts = shared(part, "kv_1")
    part = jnp.sum(parts, axis=0)
    packed = call(
        attend_kernel,
        "attend",
        (72, 128),
        BF16,
        pair,
        part,
        turn,
        keys,
        values,
        cache,
        scalars=1,
    )
    packed = call(merge_kernel, "merge", (72, 128), BF16, shared(packed, "kv_1"))
    block = call(
        project_kernel,
        "project",
        (2, 128),
        BF16,
        tp,
        shared(packed, "kv_0"),
        lam,
        head,
        out_weight,
        own,
        scalars=1,
        scratch=[pltpu.VMEM((64, 128), F32)],
    )
    pieces = shared(block, KV_TP).reshape(256, 128)
    partial = call(
        mlp_kernel,
        "mlp",
        (128, 128),
        F32,
        at,
        pieces,
        mlp_gain.reshape(1, 4096),
        gate_weight,
        up_weight,
        down_weight,
        scalars=1,
        scratch=[pltpu.VMEM((128, 128), F32), pltpu.VMEM((128, 128), F32)],
    )
    sums = lax.all_to_all(partial.reshape(128, 1, 128), KV_TP, 0, 0, tiled=True)
    return call(total_kernel, "total", (4, 32), BF16, sums.reshape(128, 128))


def solution(mesh):
    torus = Mesh(
        mesh.devices.reshape(mesh.shape["dp"], 8, 8, mesh.shape["tp"]), ("dp", "kv_0", "kv_1", "tp")
    )
    in_specs = (
        P("dp", KV_TP),
        P(),
        P(KV, "tp"),
        P("dp", KV, "tp", None),
        P("dp", KV, "tp", None),
        P("tp"),
        P(),
        P(KV, "tp"),
        P(),
        P(KV_TP, None),
        P(KV_TP, None),
        P(KV_TP, None),
    )
    out_specs = P("dp", KV_TP)
    return jax.shard_map(
        shards, mesh=torus, in_specs=in_specs, out_specs=out_specs, check_vma=False
    )
```

```python
import jax
import jax.numpy as jnp
import numpy as np
from jax import lax
from jax.experimental import pallas as pl
from jax.experimental.pallas import tpu as pltpu
from jax.sharding import Mesh
from jax.sharding import PartitionSpec as P

KV = ("kv_0", "kv_1")
KV_TP = ("kv_0", "kv_1", "tp")
EPS = 1e-06
THETA = 10000.0
F32 = jnp.float32
BF16 = jnp.bfloat16
SHAPE = jax.ShapeDtypeStruct


def lanes(shape):
    return lax.broadcasted_iota(jnp.int32, shape, len(shape) - 1)


def rows(shape):
    return lax.broadcasted_iota(jnp.int32, shape, len(shape) - 2)


def inner_last(left, right):
    return lax.dot_general(left, right, (((1,), (1,)), ((), ())), preferred_element_type=F32)


def shared(block, axis):
    copies = jnp.broadcast_to(block, (lax.axis_size(axis), *block.shape))
    return lax.all_to_all(copies, axis, 0, 0, tiled=True)


def prepare_kernel(
    kv_ref, own_in, weight_in, gain_in, lam_in, turn_in, head_in, key_in, value_in,
    own_ref, weight_ref, gain_ref, lam_ref, turn_ref, head_ref, cache_ref, all_ref, row_ref, sems,
):
    away = pl.ds(2 - 2 * (kv_ref[0] // 8 % 2), 2)
    pairs = [
        (weight_in, weight_ref), (key_in.at[away], cache_ref.at[0:2]),
        (value_in.at[away], cache_ref.at[2:4]), (own_in, own_ref), (gain_in, all_ref),
        (lam_in, row_ref), (turn_in, turn_ref), (head_in, head_ref),
    ]
    copies = [pltpu.make_async_copy(a, b, sems.at[k]) for k, (a, b) in enumerate(pairs)]
    for copy in copies:
        copy.start()
    for copy in copies[3:]:
        copy.wait()
    line = all_ref[pl.ds(kv_ref[0] // 2, 1), :]
    gain_ref[...] = jnp.where(kv_ref[0] % 2 == 0, line, pltpu.roll(line, 64, 1))
    picked = jnp.where(lanes((32, 16)) == rows((32, 16)) // 2, row_ref[...], 0.0)
    lam_ref[...] = jnp.broadcast_to(jnp.sum(picked, axis=1, keepdims=True), (32, 128))
    for copy in copies[:3]:
        copy.wait()


def query_kernel(both_ref, gain_ref, weight_ref, out_ref):
    x = jnp.concatenate([both_ref[0], both_ref[1]], axis=1).astype(F32)
    square = jnp.sum(x * x, axis=1, keepdims=True)
    scaled = (x * gain_ref[:, :64]).astype(BF16)
    q = jnp.dot(scaled, weight_ref[...], preferred_element_type=F32)
    wide = jnp.broadcast_to(square, (4, 128))
    for pair in range(2):
        two = slice(2 * pair, 2 * pair + 2)
        for h in range(16):
            out_ref[pair, 2 * h : 2 * h + 2, :] = q[two, 128 * h : 128 * h + 128]
        for k in range(4):
            out_ref[pair, 32 + 2 * k : 34 + 2 * k, :] = wide[two]


def pack(values, lse):
    high = lse.astype(BF16).astype(F32)
    mid = (lse - high).astype(BF16).astype(F32)
    low = lse - high - mid
    at = rows((8, 128))
    tail = jnp.where(at == 0, high, jnp.where(at == 1, mid, jnp.where(at == 2, low, 0.0)))
    return values.astype(BF16), tail.astype(BF16)


def attend_kernel(pair_ref, part_ref, turn_ref, key_ref, value_ref, cache_ref, out_ref):
    total = part_ref[...]
    scale = lax.rsqrt(total[32:40] * (1.0 / 4096) + EPS)
    q = (total[:32].reshape(4, 8, 128) * scale[None]).reshape(32, 128)
    lane = lanes((32, 128))
    swapped = jnp.where(lane % 64 < 32, pltpu.roll(q, 96, 1), pltpu.roll(q, 32, 1))
    turned = q * turn_ref[0:1] + swapped * turn_ref[1:2]
    both = jnp.concatenate(
        [jnp.where(lane < 64, turned, 0.0), jnp.where(lane < 64, 0.0, turned)], axis=0
    ).astype(BF16)
    here = 2 * pair_ref[0]

    def against(b):
        near = inner_last(both, key_ref[here + b])
        return jnp.concatenate([near, inner_last(both, cache_ref[b])], axis=1)

    scores = jnp.where(rows((64, 512)) % 2 == 0, against(0), against(1)) * 0.125
    peak = jnp.max(scores, axis=1, keepdims=True)
    e = jnp.exp(scores - peak)
    total_e = jnp.sum(e, axis=1, keepdims=True)
    probs = e.astype(BF16)

    def valued(b):
        near = jnp.dot(probs[:, :256], value_ref[here + b], preferred_element_type=F32)
        return near + jnp.dot(probs[:, 256:], cache_ref[2 + b], preferred_element_type=F32)

    value = jnp.where(rows((64, 128)) % 2 == 0, valued(0), valued(1)) / total_e
    lse = peak + jnp.log(total_e)
    eye = rows((64, 128)) == lanes((64, 128))
    lse_row = jnp.sum(jnp.where(eye, lse, 0.0), axis=0, keepdims=True)
    out_ref[:64, :], out_ref[64:, :] = pack(value, lse_row)


def lse_of(parts_ref):
    tails = []
    for k in range(8):
        tail = parts_ref[k, 64:, :].astype(F32)
        tails.append(tail[0:1] + tail[1:2] + tail[2:3])
    return jnp.concatenate(tails, axis=0)


def weighed(parts_ref, share, slots):
    value = 0.0
    for k in slots:
        value = value + share[:64, k : k + 1] * parts_ref[k, :64, :].astype(F32)
    return value


def merge_kernel(parts_ref, out_ref):
    lse = lse_of(parts_ref)
    peak = jnp.max(lse, axis=0, keepdims=True)
    e = jnp.exp(lse - peak)
    total = jnp.sum(e, axis=0, keepdims=True)
    value = weighed(parts_ref, (e / total).T, range(8))
    out_ref[:64, :], out_ref[64:, :] = pack(value, peak + jnp.log(total))


def project_kernel(tp_ref, parts_ref, lam_ref, gain_ref, weight_ref, own_ref, out_ref, heads_ref):
    lse = lse_of(parts_ref)
    even = rows((8, 128)) % 2 == 0
    low = jnp.finfo(F32).min
    peak = jnp.where(
        even,
        jnp.max(jnp.where(even, lse, low), axis=0, keepdims=True),
        jnp.max(jnp.where(even, low, lse), axis=0, keepdims=True),
    )
    e = jnp.exp(lse - peak)
    total = jnp.where(
        even,
        jnp.sum(jnp.where(even, e, 0.0), axis=0, keepdims=True),
        jnp.sum(jnp.where(even, 0.0, e), axis=0, keepdims=True),
    )
    share = (e / total).T
    for pair in range(2):
        value = weighed(parts_ref, share, range(pair, 8, 2))
        difference = value[:32] - lam_ref[...] * value[32:]
        norm = lax.rsqrt(jnp.mean(difference * difference, axis=1, keepdims=True) + EPS)
        heads_ref[32 * pair : 32 * pair + 32, :] = difference * norm * gain_ref[...]
    head_out = jnp.concatenate(
        [
            jnp.concatenate(
                [heads_ref[32 * pair + 2 * h : 32 * pair + 2 * h + 2, :] for h in range(16)], axis=1
            )
            for pair in range(2)
        ],
        axis=0,
    )
    part = inner_last(head_out.astype(BF16), weight_ref[...])
    part = part.astype(BF16).astype(F32)
    lane = lanes((4, 64))
    own = own_ref[...].astype(F32)
    part = part + jnp.where(lane // 32 == tp_ref[0], jnp.concatenate([own, own], axis=1), 0.0)
    out_ref[...] = jnp.concatenate([part[0:2], part[2:4]], axis=1).astype(BF16)


def mlp_kernel(
    at_ref, pieces_ref, gain_ref, gate_ref, up_ref, down_ref, out_ref, tile_ref, row_ref
):
    y = pieces_ref[...].astype(F32).reshape(32, 8, 128)
    lane = lanes((32, 8, 128))
    s = y + pltpu.roll(y, 6, 1)
    far = pltpu.roll(s, 4, 1)
    front = jnp.where(lane < 64, s, pltpu.roll(far, 64, 2))
    back = jnp.where(lane < 64, pltpu.roll(s, 64, 2), far)
    four = jnp.where(rows((32, 8, 128)) < 2, front, pltpu.roll(back, 2, 1))
    stream = jnp.concatenate([four[v, 0:4] for v in range(32)], axis=1)
    square = jnp.sum(stream * stream, axis=1, keepdims=True) * (1.0 / 4096)
    normed = (stream * lax.rsqrt(square + EPS) * gain_ref[...]).astype(BF16)
    gate = inner_last(normed, gate_ref[...])
    up = inner_last(normed, up_ref[...])
    hidden = (gate / (1.0 + jnp.exp(-gate)) * up).astype(BF16)
    down = jnp.dot(hidden, down_ref[...], preferred_element_type=F32)
    down = down + jnp.where(lanes((4, 4096)) // 32 == at_ref[0], stream, 0.0)
    for v in range(32):
        tile_ref[4 * v : 4 * v + 4, :] = down[:, 128 * v : 128 * v + 128]
    by_row = [tile_ref[pl.ds(r, 32, stride=4), :] for r in range(4)]
    wide = lanes((32, 128)) // 32
    for g in range(4):
        line = by_row[g]
        for r in range(4):
            if r != g:
                line = jnp.where(wide == r, pltpu.roll(by_row[r], (r - g) % 4 * 32, 1), line)
        row_ref[pl.ds(g, 32, stride=4), :] = line
    out_ref[...] = row_ref[...]


def total_kernel(parts_ref, out_ref):
    line = jnp.sum(parts_ref[...], axis=0, keepdims=True)
    out_ref[...] = jnp.concatenate(
        [line[:, 32 * r : 32 * r + 32] for r in range(4)], axis=0
    ).astype(BF16)


def call(kernel, name, shape, dtype, *args, scalars=0, scratch=()):
    smem = pl.BlockSpec(memory_space=pltpu.SMEM)
    vmem = pl.BlockSpec(memory_space=pltpu.VMEM)
    near = [pltpu.with_memory_space_constraint(x, pltpu.VMEM) for x in args[scalars:]]
    return pl.pallas_call(
        kernel,
        out_shape=pltpu.VMEM(shape, dtype) if name != "total" else SHAPE(shape, dtype),
        in_specs=[smem] * scalars + [vmem] * len(near),
        out_specs=vmem,
        scratch_shapes=list(scratch),
    )(*args[:scalars], *near)


def turn_tables(position):
    inverse = np.power(THETA, -np.arange(32, dtype=np.float64) / 32).astype(np.float32)
    angles = (np.float32(position) * inverse).astype(np.float64)
    cos = np.tile(np.cos(angles), 4)
    sin = np.tile(np.concatenate([-np.sin(angles), np.sin(angles)]), 2)
    return jnp.asarray(np.stack([cos, sin] + [np.zeros(128)] * 6).astype(np.float32))


def shards(
    tokens,
    attn_gain,
    query_weight,
    key_cache,
    value_cache,
    head_lambda,
    head_gain,
    out_weight,
    mlp_gain,
    gate_weight,
    up_weight,
    down_weight,
):
    tp = lax.axis_index("tp").astype(jnp.int32).reshape(1)
    kv = lax.axis_index(KV)
    at = lax.axis_index(KV_TP).astype(jnp.int32).reshape(1)
    turn = turn_tables(key_cache.shape[1] * lax.axis_size(KV))
    keys = key_cache.reshape(4, 256, 128)
    values = value_cache.reshape(4, 256, 128)
    pair = (kv // 8 % 2).astype(jnp.int32).reshape(1)
    own, weight, gain, lam, turn, head, cache = pl.pallas_call(
        prepare_kernel,
        name="prepare",
        out_shape=[
            pltpu.VMEM((4, 32), BF16),
            pltpu.VMEM((64, 2048), BF16),
            pltpu.VMEM((1, 128), F32),
            pltpu.VMEM((32, 128), F32),
            pltpu.VMEM((8, 128), F32),
            pltpu.VMEM((1, 128), F32),
            pltpu.VMEM((4, 256, 128), BF16),
        ],
        in_specs=[pl.BlockSpec(memory_space=pltpu.SMEM)] + [pl.BlockSpec(memory_space=pl.ANY)] * 8,
        out_specs=[pl.BlockSpec(memory_space=pltpu.VMEM)] * 7,
        scratch_shapes=[
            pltpu.VMEM((32, 128), F32),
            pltpu.VMEM((1, 16), F32),
            pltpu.SemaphoreType.DMA((8,)),
        ],
    )(
        kv.astype(jnp.int32).reshape(1),
        tokens,
        query_weight,
        attn_gain.reshape(32, 128),
        head_lambda.reshape(1, 16),
        turn,
        head_gain.reshape(1, 128),
        keys,
        values,
    )
    both = lax.all_gather(own, "tp")
    part = call(query_kernel, "query", (2, 40, 128), F32, both, gain, weight)
    part, at, pair = lax.optimization_barrier((part, at, pair))
    copies = jnp.broadcast_to(part[None], (4, 2, 40, 128)).reshape(8, 40, 128)
    part = jnp.sum(lax.all_to_all(copies, "kv_0", 0, 0, tiled=True), axis=0)
    part, cache = lax.optimization_barrier((part, cache))
    cache = lax.ppermute(cache, "kv_0", [(z, z ^ 1) for z in range(8)])
    parts = shared(part, "kv_1")
    part = jnp.sum(parts, axis=0)
    packed = call(
        attend_kernel,
        "attend",
        (72, 128),
        BF16,
        pair,
        part,
        turn,
        keys,
        values,
        cache,
        scalars=1,
    )
    packed = call(merge_kernel, "merge", (72, 128), BF16, shared(packed, "kv_1"))
    block = call(
        project_kernel,
        "project",
        (2, 128),
        BF16,
        tp,
        shared(packed, "kv_0"),
        lam,
        head,
        out_weight,
        own,
        scalars=1,
        scratch=[pltpu.VMEM((64, 128), F32)],
    )
    pieces = shared(block, KV_TP).reshape(256, 128)
    partial = call(
        mlp_kernel,
        "mlp",
        (128, 128),
        F32,
        at,
        pieces,
        mlp_gain.reshape(1, 4096),
        gate_weight,
        up_weight,
        down_weight,
        scalars=1,
        scratch=[pltpu.VMEM((128, 128), F32), pltpu.VMEM((128, 128), F32)],
    )
    sums = lax.all_to_all(partial.reshape(128, 1, 128), KV_TP, 0, 0, tiled=True)
    return call(total_kernel, "total", (4, 32), BF16, sums.reshape(128, 128))


def solution(mesh):
    torus = Mesh(
        mesh.devices.reshape(mesh.shape["dp"], 8, 8, mesh.shape["tp"]), ("dp", "kv_0", "kv_1", "tp")
    )
    in_specs = (
        P("dp", KV_TP),
        P(),
        P(KV, "tp"),
        P("dp", KV, "tp", None),
        P("dp", KV, "tp", None),
        P("tp"),
        P(),
        P(KV, "tp"),
        P(),
        P(KV_TP, None),
        P(KV_TP, None),
        P(KV_TP, None),
    )
    out_specs = P("dp", KV_TP)
    return jax.shard_map(
        shards, mesh=torus, in_specs=in_specs, out_specs=out_specs, check_vma=False
    )
```

```python
import jax
import jax.numpy as jnp
import numpy as np
from jax import lax
from jax.experimental import pallas as pl
from jax.experimental.pallas import tpu as pltpu
from jax.sharding import Mesh
from jax.sharding import PartitionSpec as P

KV = ("kv_0", "kv_1")
KV_TP = ("kv_0", "kv_1", "tp")
EPS = 1e-06
THETA = 10000.0
F32 = jnp.float32
BF16 = jnp.bfloat16
SHAPE = jax.ShapeDtypeStruct


def lanes(shape):
    return lax.broadcasted_iota(jnp.int32, shape, len(shape) - 1)


def rows(shape):
    return lax.broadcasted_iota(jnp.int32, shape, len(shape) - 2)


def inner_last(left, right):
    return lax.dot_general(left, right, (((1,), (1,)), ((), ())), preferred_element_type=F32)


def shared(block, axis):
    copies = jnp.broadcast_to(block, (lax.axis_size(axis), *block.shape))
    return lax.all_to_all(copies, axis, 0, 0, tiled=True)


def prepare_kernel(
    kv_ref, own_in, weight_in, gain_in, lam_in, turn_in, head_in,
    own_ref, weight_ref, gain_ref, lam_ref, turn_ref, head_ref, all_ref, row_ref, sems,
):
    pairs = [
        (weight_in, weight_ref), (own_in, own_ref), (gain_in, all_ref), (lam_in, row_ref),
        (turn_in, turn_ref), (head_in, head_ref),
    ]
    copies = [pltpu.make_async_copy(a, b, sems.at[k]) for k, (a, b) in enumerate(pairs)]
    for copy in copies:
        copy.start()
    for copy in copies[1:]:
        copy.wait()
    line = all_ref[pl.ds(kv_ref[0] // 2, 1), :]
    gain_ref[...] = jnp.where(kv_ref[0] % 2 == 0, line, pltpu.roll(line, 64, 1))
    picked = jnp.where(lanes((32, 16)) == rows((32, 16)) // 2, row_ref[...], 0.0)
    lam_ref[...] = jnp.broadcast_to(jnp.sum(picked, axis=1, keepdims=True), (32, 128))
    copies[0].wait()


def swap_kernel(pair_ref, key_ref, value_ref, out_ref):
    away = 2 - 2 * pair_ref[0]
    for b in range(2):
        out_ref[b] = key_ref[away + b]
        out_ref[2 + b] = value_ref[away + b]


def query_kernel(both_ref, gain_ref, weight_ref, out_ref):
    x = jnp.concatenate([both_ref[0], both_ref[1]], axis=1).astype(F32)
    square = jnp.sum(x * x, axis=1, keepdims=True)
    scaled = (x * gain_ref[:, :64]).astype(BF16)
    q = jnp.dot(scaled, weight_ref[...], preferred_element_type=F32)
    wide = jnp.broadcast_to(square, (4, 128))
    for pair in range(2):
        two = slice(2 * pair, 2 * pair + 2)
        for h in range(16):
            out_ref[pair, 2 * h : 2 * h + 2, :] = q[two, 128 * h : 128 * h + 128]
        for k in range(4):
            out_ref[pair, 32 + 2 * k : 34 + 2 * k, :] = wide[two]


def pack(values, lse):
    high = lse.astype(BF16).astype(F32)
    mid = (lse - high).astype(BF16).astype(F32)
    low = lse - high - mid
    at = rows((8, 128))
    tail = jnp.where(at == 0, high, jnp.where(at == 1, mid, jnp.where(at == 2, low, 0.0)))
    return values.astype(BF16), tail.astype(BF16)


def attend_kernel(pair_ref, part_ref, turn_ref, key_ref, value_ref, cache_ref, out_ref):
    total = part_ref[...]
    scale = lax.rsqrt(total[32:40] * (1.0 / 4096) + EPS)
    q = (total[:32].reshape(4, 8, 128) * scale[None]).reshape(32, 128)
    lane = lanes((32, 128))
    swapped = jnp.where(lane % 64 < 32, pltpu.roll(q, 96, 1), pltpu.roll(q, 32, 1))
    turned = q * turn_ref[0:1] + swapped * turn_ref[1:2]
    both = jnp.concatenate(
        [jnp.where(lane < 64, turned, 0.0), jnp.where(lane < 64, 0.0, turned)], axis=0
    ).astype(BF16)
    here = 2 * pair_ref[0]

    def against(b):
        near = inner_last(both, key_ref[here + b])
        return jnp.concatenate([near, inner_last(both, cache_ref[b])], axis=1)

    scores = jnp.where(rows((64, 512)) % 2 == 0, against(0), against(1)) * 0.125
    peak = jnp.max(scores, axis=1, keepdims=True)
    e = jnp.exp(scores - peak)
    total_e = jnp.sum(e, axis=1, keepdims=True)
    probs = e.astype(BF16)

    def valued(b):
        near = jnp.dot(probs[:, :256], value_ref[here + b], preferred_element_type=F32)
        return near + jnp.dot(probs[:, 256:], cache_ref[2 + b], preferred_element_type=F32)

    value = jnp.where(rows((64, 128)) % 2 == 0, valued(0), valued(1)) / total_e
    lse = peak + jnp.log(total_e)
    eye = rows((64, 128)) == lanes((64, 128))
    lse_row = jnp.sum(jnp.where(eye, lse, 0.0), axis=0, keepdims=True)
    out_ref[:64, :], out_ref[64:, :] = pack(value, lse_row)


def lse_of(parts_ref):
    tails = []
    for k in range(8):
        tail = parts_ref[k, 64:, :].astype(F32)
        tails.append(tail[0:1] + tail[1:2] + tail[2:3])
    return jnp.concatenate(tails, axis=0)


def weighed(parts_ref, share, slots):
    value = 0.0
    for k in slots:
        value = value + share[:64, k : k + 1] * parts_ref[k, :64, :].astype(F32)
    return value


def merge_kernel(parts_ref, out_ref):
    lse = lse_of(parts_ref)
    peak = jnp.max(lse, axis=0, keepdims=True)
    e = jnp.exp(lse - peak)
    total = jnp.sum(e, axis=0, keepdims=True)
    value = weighed(parts_ref, (e / total).T, range(8))
    out_ref[:64, :], out_ref[64:, :] = pack(value, peak + jnp.log(total))


def project_kernel(tp_ref, parts_ref, lam_ref, gain_ref, weight_ref, own_ref, out_ref, heads_ref):
    lse = lse_of(parts_ref)
    even = rows((8, 128)) % 2 == 0
    low = jnp.finfo(F32).min
    peak = jnp.where(
        even,
        jnp.max(jnp.where(even, lse, low), axis=0, keepdims=True),
        jnp.max(jnp.where(even, low, lse), axis=0, keepdims=True),
    )
    e = jnp.exp(lse - peak)
    total = jnp.where(
        even,
        jnp.sum(jnp.where(even, e, 0.0), axis=0, keepdims=True),
        jnp.sum(jnp.where(even, 0.0, e), axis=0, keepdims=True),
    )
    share = (e / total).T
    for pair in range(2):
        value = weighed(parts_ref, share, range(pair, 8, 2))
        difference = value[:32] - lam_ref[...] * value[32:]
        norm = lax.rsqrt(jnp.mean(difference * difference, axis=1, keepdims=True) + EPS)
        heads_ref[32 * pair : 32 * pair + 32, :] = difference * norm * gain_ref[...]
    head_out = jnp.concatenate(
        [
            jnp.concatenate(
                [heads_ref[32 * pair + 2 * h : 32 * pair + 2 * h + 2, :] for h in range(16)], axis=1
            )
            for pair in range(2)
        ],
        axis=0,
    )
    part = inner_last(head_out.astype(BF16), weight_ref[...])
    part = part.astype(BF16).astype(F32)
    lane = lanes((4, 64))
    own = own_ref[...].astype(F32)
    part = part + jnp.where(lane // 32 == tp_ref[0], jnp.concatenate([own, own], axis=1), 0.0)
    out_ref[...] = jnp.concatenate([part[0:2], part[2:4]], axis=1).astype(BF16)


def mlp_kernel(
    at_ref, pieces_ref, gain_ref, gate_ref, up_ref, down_ref, out_ref, tile_ref, row_ref
):
    y = pieces_ref[...].astype(F32).reshape(32, 8, 128)
    lane = lanes((32, 8, 128))
    s = y + pltpu.roll(y, 6, 1)
    far = pltpu.roll(s, 4, 1)
    front = jnp.where(lane < 64, s, pltpu.roll(far, 64, 2))
    back = jnp.where(lane < 64, pltpu.roll(s, 64, 2), far)
    four = jnp.where(rows((32, 8, 128)) < 2, front, pltpu.roll(back, 2, 1))
    stream = jnp.concatenate([four[v, 0:4] for v in range(32)], axis=1)
    square = jnp.sum(stream * stream, axis=1, keepdims=True) * (1.0 / 4096)
    normed = (stream * lax.rsqrt(square + EPS) * gain_ref[...]).astype(BF16)
    gate = inner_last(normed, gate_ref[...])
    up = inner_last(normed, up_ref[...])
    hidden = (gate / (1.0 + jnp.exp(-gate)) * up).astype(BF16)
    down = jnp.dot(hidden, down_ref[...], preferred_element_type=F32)
    down = down + jnp.where(lanes((4, 4096)) // 32 == at_ref[0], stream, 0.0)
    for v in range(32):
        tile_ref[4 * v : 4 * v + 4, :] = down[:, 128 * v : 128 * v + 128]
    by_row = [tile_ref[pl.ds(r, 32, stride=4), :] for r in range(4)]
    wide = lanes((32, 128)) // 32
    for g in range(4):
        line = by_row[g]
        for r in range(4):
            if r != g:
                line = jnp.where(wide == r, pltpu.roll(by_row[r], (r - g) % 4 * 32, 1), line)
        row_ref[pl.ds(g, 32, stride=4), :] = line
    out_ref[...] = row_ref[...]


def total_kernel(parts_ref, out_ref):
    line = jnp.sum(parts_ref[...], axis=0, keepdims=True)
    out_ref[...] = jnp.concatenate(
        [line[:, 32 * r : 32 * r + 32] for r in range(4)], axis=0
    ).astype(BF16)


def call(kernel, name, shape, dtype, *args, scalars=0, scratch=()):
    smem = pl.BlockSpec(memory_space=pltpu.SMEM)
    vmem = pl.BlockSpec(memory_space=pltpu.VMEM)
    near = [pltpu.with_memory_space_constraint(x, pltpu.VMEM) for x in args[scalars:]]
    return pl.pallas_call(
        kernel,
        out_shape=pltpu.VMEM(shape, dtype) if name != "total" else SHAPE(shape, dtype),
        in_specs=[smem] * scalars + [vmem] * len(near),
        out_specs=vmem,
        scratch_shapes=list(scratch),
    )(*args[:scalars], *near)


def turn_tables(position):
    inverse = np.power(THETA, -np.arange(32, dtype=np.float64) / 32).astype(np.float32)
    angles = (np.float32(position) * inverse).astype(np.float64)
    cos = np.tile(np.cos(angles), 4)
    sin = np.tile(np.concatenate([-np.sin(angles), np.sin(angles)]), 2)
    return jnp.asarray(np.stack([cos, sin] + [np.zeros(128)] * 6).astype(np.float32))


def shards(
    tokens,
    attn_gain,
    query_weight,
    key_cache,
    value_cache,
    head_lambda,
    head_gain,
    out_weight,
    mlp_gain,
    gate_weight,
    up_weight,
    down_weight,
):
    tp = lax.axis_index("tp").astype(jnp.int32).reshape(1)
    kv = lax.axis_index(KV)
    at = lax.axis_index(KV_TP).astype(jnp.int32).reshape(1)
    turn = turn_tables(key_cache.shape[1] * lax.axis_size(KV))
    keys = key_cache.reshape(4, 256, 128)
    values = value_cache.reshape(4, 256, 128)
    pair = (kv // 8 % 2).astype(jnp.int32).reshape(1)
    own, weight, gain, lam, turn, head = pl.pallas_call(
        prepare_kernel,
        name="prepare",
        out_shape=[
            pltpu.VMEM((4, 32), BF16),
            pltpu.VMEM((64, 2048), BF16),
            pltpu.VMEM((1, 128), F32),
            pltpu.VMEM((32, 128), F32),
            pltpu.VMEM((8, 128), F32),
            pltpu.VMEM((1, 128), F32),
        ],
        in_specs=[pl.BlockSpec(memory_space=pltpu.SMEM)] + [pl.BlockSpec(memory_space=pl.ANY)] * 6,
        out_specs=[pl.BlockSpec(memory_space=pltpu.VMEM)] * 6,
        scratch_shapes=[
            pltpu.VMEM((32, 128), F32),
            pltpu.VMEM((1, 16), F32),
            pltpu.SemaphoreType.DMA((6,)),
        ],
    )(
        kv.astype(jnp.int32).reshape(1),
        tokens,
        query_weight,
        attn_gain.reshape(32, 128),
        head_lambda.reshape(1, 16),
        turn,
        head_gain.reshape(1, 128),
    )
    both = lax.all_gather(own, "tp")
    part = call(query_kernel, "query", (2, 40, 128), F32, both, gain, weight)
    part, at, pair = lax.optimization_barrier((part, at, pair))
    copies = jnp.broadcast_to(part[None], (4, 2, 40, 128)).reshape(8, 40, 128)
    part = jnp.sum(lax.all_to_all(copies, "kv_0", 0, 0, tiled=True), axis=0)
    part, pair = lax.optimization_barrier((part, pair))
    cache = call(swap_kernel, "swap", (4, 256, 128), BF16, pair, keys, values, scalars=1)
    part, cache = lax.optimization_barrier((part, cache))
    cache = lax.ppermute(cache, "kv_0", [(z, z ^ 1) for z in range(8)])
    parts = shared(part, "kv_1")
    part = jnp.sum(parts, axis=0)
    packed = call(
        attend_kernel,
        "attend",
        (72, 128),
        BF16,
        pair,
        part,
        turn,
        keys,
        values,
        cache,
        scalars=1,
    )
    packed = call(merge_kernel, "merge", (72, 128), BF16, shared(packed, "kv_1"))
    block = call(
        project_kernel,
        "project",
        (2, 128),
        BF16,
        tp,
        shared(packed, "kv_0"),
        lam,
        head,
        out_weight,
        own,
        scalars=1,
        scratch=[pltpu.VMEM((64, 128), F32)],
    )
    pieces = shared(block, KV_TP).reshape(256, 128)
    partial = call(
        mlp_kernel,
        "mlp",
        (128, 128),
        F32,
        at,
        pieces,
        mlp_gain.reshape(1, 4096),
        gate_weight,
        up_weight,
        down_weight,
        scalars=1,
        scratch=[pltpu.VMEM((128, 128), F32), pltpu.VMEM((128, 128), F32)],
    )
    sums = lax.all_to_all(partial.reshape(128, 1, 128), KV_TP, 0, 0, tiled=True)
    return call(total_kernel, "total", (4, 32), BF16, sums.reshape(128, 128))


def solution(mesh):
    torus = Mesh(
        mesh.devices.reshape(mesh.shape["dp"], 8, 8, mesh.shape["tp"]), ("dp", "kv_0", "kv_1", "tp")
    )
    in_specs = (
        P("dp", KV_TP),
        P(),
        P(KV, "tp"),
        P("dp", KV, "tp", None),
        P("dp", KV, "tp", None),
        P("tp"),
        P(),
        P(KV, "tp"),
        P(),
        P(KV_TP, None),
        P(KV_TP, None),
        P(KV_TP, None),
    )
    out_specs = P("dp", KV_TP)
    return jax.shard_map(
        shards, mesh=torus, in_specs=in_specs, out_specs=out_specs, check_vma=False
    )
```
